512 devices in a mesh: rep: 2 (over z_hi), fs: 32 (over z_lo, y), tp: 8 (over x, core).
Axes of the slice: x: 4, y: 4, z: 16 (z_hi: 2, z_lo: 8; z = z_hi * 8 + z_lo), core: 2. Of those that a mesh axis runs over, the one named last changes fastest.
Arguments:
- incoming_features: bfloat16 [12288, 2048], P(('rep', 'fs'), 'tp'), may hold values from -6 to 6
- attend_prenormal_scale: bfloat16 [2048], replicated, may hold values from 0.099609375 to 1.8984375
- probe_matrix: bfloat16 [2048, 512], P('fs', 'tp'), may hold values from -0.125 to 0.125
- lookup_matrix: bfloat16 [2048, 512], P('fs', 'tp'), may hold values from -0.125 to 0.125
- content_matrix: bfloat16 [2048, 1024], P('fs', 'tp'), may hold values from -0.125 to 0.125
- forgetting_matrix: bfloat16 [2048, 512], P('fs', 'tp'), may hold values from -0.125 to 0.125
- result_switch_matrix: bfloat16 [2048, 1024], P('fs', 'tp'), may hold values from -0.125 to 0.125
- forgetting_shift: float32 [512], P('tp'), may hold values from -0.5 to 5.5
- spike_forget_logarithm: float32 [12288, 512], P(('rep', 'fs'), 'tp'), may hold values from -0.7 to 0
- attend_unit_scale: bfloat16 [1024], P('tp'), may hold values from 0.099609375 to 1.8984375
- attend_result_matrix: bfloat16 [1024, 2048], P('tp', 'fs'), may hold values from -0.1875 to 0.1875
- perceptron_scale: bfloat16 [2048], replicated, may hold values from 0.099609375 to 1.8984375
- content_expand_matrix: bfloat16 [2048, 4096], P('fs', 'tp'), may hold values from -0.125 to 0.125
- switch_expand_matrix: bfloat16 [2048, 4096], P('fs', 'tp'), may hold values from -0.125 to 0.125
- content_kernel: bfloat16 [3, 4096], P(None, 'tp'), may hold values from -3.5 to 3.5
- switch_kernel: bfloat16 [3, 4096], P(None, 'tp'), may hold values from -3.5 to 3.5
- contract_matrix: bfloat16 [4096, 2048], P('tp', 'fs'), may hold values from -0.09375 to 0.09375
Outputs:
- out_rows: bfloat16 [12288, 2048], P(('rep', 'fs'), 'tp')
The draws below stay inside these ranges and needn't reach their ends.
All inputs are finite; a program needn't handle non-finite values.
Results may differ from the reference program's by a relative error of at most 0.02.
Values may be sent and summed in bfloat16 or wider, within the bound.
A program may use at most 64 MiB of HBM per device.

```python
import math
import jax
import jax.numpy as jnp
from jax import lax

EMBED_DIM = 2048
HEAD_K = 32
HEAD_V = 64
FF = 4096
BLOCK = 64
CONTEXT_SPAN = 192
LOOKUP_FEATURES = 512
VAL_W = 1024
BATCH_SIZE = 64
TOKENS = 12288
N_TP = 8


def draw_forgetting_shift(key, part):
    head_count = LOOKUP_FEATURES // HEAD_K
    key_slow, key_high, key_low = jax.random.split(jax.random.fold_in(key, 11), 3)
    slow = jax.random.uniform(key_slow, (head_count,)) < 0.5
    slow_channels = jnp.repeat(slow, HEAD_K)
    high = jax.random.uniform(key_high, (LOOKUP_FEATURES,), jnp.float32, 3.5, 5.5)
    low = jax.random.uniform(key_low, (LOOKUP_FEATURES,), jnp.float32, -0.5, 1.0)
    return jnp.where(slow_channels, high, low).astype(jnp.float32)


def draw_spike_forget_logarithm(key, part):
    head_count = LOOKUP_FEATURES // HEAD_K
    key_hit, key_depth = jax.random.split(jax.random.fold_in(key, 23))
    hits = jax.random.uniform(key_hit, (TOKENS, head_count)) < 6.0 / CONTEXT_SPAN
    depth = jax.random.uniform(key_depth, (TOKENS, head_count), jnp.float32, math.log(0.5), math.log(0.8))
    return jnp.repeat(jnp.where(hits, depth, 0.0), HEAD_K, axis=1).astype(jnp.float32)


def level_of(own_key, shape, pieces, smallest, top_value):
    factor_of, own = 1.0, jax.random.fold_in(own_key, 6)
    for position, parts in pieces:
        steps = jnp.exp(jax.random.uniform(jax.random.fold_in(own, position), (parts,), jnp.float32, smallest / len(pieces), top_value / len(pieces)))
        factor_of = factor_of * jnp.repeat(steps, shape[position] // parts).reshape([-1 if axis == position else 1 for axis in range(len(shape))])
    return factor_of


def gaussian(own_key, dims, spread, limit, cuts=(), held_as=jnp.bfloat16):
    factor_of = level_of(own_key, dims, cuts, -0.22, 0.18) if cuts else 1.0
    values = jax.random.normal(own_key, dims, jnp.float32) * spread * factor_of
    return jnp.minimum(jnp.maximum(values, -limit), limit).astype(held_as)


def setup_inputs(seed: int = 0) -> dict:
    streams_of = jax.random.split(jax.random.key(seed), 18)
    incoming_features = gaussian(streams_of[0], (TOKENS, EMBED_DIM), 1.0, 6.0, ((0, 64), (1, 8)))
    attend_prenormal_scale = jnp.clip(1.0 + 0.18 * jax.random.normal(streams_of[1], (EMBED_DIM,), jnp.float32), 0.099609375, 1.8984375).astype(jnp.bfloat16)
    probe_matrix = gaussian(streams_of[2], (EMBED_DIM, LOOKUP_FEATURES), EMBED_DIM ** -0.5, 0.125, ((0, 32), (1, 8)))
    lookup_matrix = gaussian(streams_of[3], (EMBED_DIM, LOOKUP_FEATURES), EMBED_DIM ** -0.5, 0.125, ((0, 32), (1, 8)))
    content_matrix = gaussian(streams_of[4], (EMBED_DIM, VAL_W), EMBED_DIM ** -0.5, 0.125, ((0, 32), (1, 8)))
    forgetting_matrix = gaussian(streams_of[5], (EMBED_DIM, LOOKUP_FEATURES), EMBED_DIM ** -0.5, 0.125, ((0, 32), (1, 8)))
    result_switch_matrix = gaussian(streams_of[6], (EMBED_DIM, VAL_W), EMBED_DIM ** -0.5, 0.125, ((0, 32), (1, 8)))
    forgetting_shift = draw_forgetting_shift(jax.random.fold_in(streams_of[17], 71), 0)
    spike_forget_logarithm = draw_spike_forget_logarithm(jax.random.fold_in(streams_of[17], 71), 0)
    attend_unit_scale = jnp.clip(1.0 + 0.18 * jax.random.normal(streams_of[9], (VAL_W,), jnp.float32), 0.099609375, 1.8984375).astype(jnp.bfloat16)
    attend_result_matrix = gaussian(streams_of[10], (VAL_W, EMBED_DIM), VAL_W ** -0.5, 0.1875, ((0, 8), (1, 32)))
    perceptron_scale = jnp.clip(1.0 + 0.18 * jax.random.normal(streams_of[11], (EMBED_DIM,), jnp.float32), 0.099609375, 1.8984375).astype(jnp.bfloat16)
    content_expand_matrix = gaussian(streams_of[12], (EMBED_DIM, FF), EMBED_DIM ** -0.5, 0.125, ((0, 32), (1, 8)))
    switch_expand_matrix = gaussian(streams_of[13], (EMBED_DIM, FF), EMBED_DIM ** -0.5, 0.125, ((0, 32), (1, 8)))
    content_kernel = gaussian(streams_of[14], (3, FF), 3 ** -0.5, 3.5, ((1, 8),))
    switch_kernel = gaussian(streams_of[15], (3, FF), 3 ** -0.5, 3.5, ((1, 8),))
    contract_matrix = gaussian(streams_of[16], (FF, EMBED_DIM), FF ** -0.5, 0.09375, ((0, 8), (1, 32)))
    return {"incoming_features": incoming_features, "attend_prenormal_scale": attend_prenormal_scale, "probe_matrix": probe_matrix, "lookup_matrix": lookup_matrix, "content_matrix": content_matrix, "forgetting_matrix": forgetting_matrix, "result_switch_matrix": result_switch_matrix, "forgetting_shift": forgetting_shift, "spike_forget_logarithm": spike_forget_logarithm, "attend_unit_scale": attend_unit_scale, "attend_result_matrix": attend_result_matrix, "perceptron_scale": perceptron_scale, "content_expand_matrix": content_expand_matrix, "switch_expand_matrix": switch_expand_matrix, "content_kernel": content_kernel, "switch_kernel": switch_kernel, "contract_matrix": contract_matrix}


norm_eps = 1e-06
switch_multiplier = 16.0

def row_norm(content_tokens, gain):
    content_tokens = content_tokens.astype(jnp.float32)
    scaled = content_tokens * lax.rsqrt(lax.optimization_barrier(jnp.mean(content_tokens * content_tokens, axis=-1, keepdims=True)) + norm_eps)
    return (scaled * gain.astype(jnp.float32)).astype(jnp.bfloat16)

def gated_scan(probe_tokens, lookup_tokens, content_tokens, forgetting_scores):
    length, heads, key_size = probe_tokens.shape
    value_size = content_tokens.shape[-1]
    blocks = length // BLOCK

    def split_blocks(array):
        return array.reshape(blocks, BLOCK, heads, array.shape[-1])
    causal = jnp.arange(BLOCK)[:, None] >= jnp.arange(BLOCK)[None, :]
    highest = lax.Precision.HIGHEST

    def step(state, incoming_tokens):
        query_block, key_block, value_block, decay_block = incoming_tokens
        cumulative = jnp.cumsum(decay_block, axis=0)
        differ = cumulative[:, None] - cumulative[None, :]
        weight = jnp.exp(jnp.where(causal[:, :, None, None], differ, -jnp.inf))
        scores = jnp.einsum('thd,shd,tshd->tsh', query_block, key_block, weight, precision=highest)
        inner = jnp.einsum('tsh,shv->thv', scores, value_block, precision=highest)
        carried = jnp.einsum('thd,hdv->thv', query_block * jnp.exp(cumulative), state, precision=highest)
        final = cumulative[-1]
        state = jnp.exp(final)[:, :, None] * state + jnp.einsum('shd,shv->hdv', key_block * jnp.exp(final[None] - cumulative), value_block, precision=highest)
        return (state, inner + carried)
    start_state = jnp.zeros((heads, key_size, value_size), jnp.float32)
    _, result_tokens = lax.scan(step, start_state, (split_blocks(probe_tokens), split_blocks(lookup_tokens), split_blocks(content_tokens), split_blocks(forgetting_scores)))
    return result_tokens.reshape(length, heads, value_size)

def attend_unit_results(probe_tokens, lookup_tokens, content_tokens, result_switch, forgetting_raw, spike_forgetting, attend_unit_scale):
    length = probe_tokens.shape[0]
    heads = probe_tokens.shape[1] // HEAD_K
    forgetting_scores = jax.nn.log_sigmoid(forgetting_raw) / switch_multiplier + spike_forgetting

    def split_heads(array, width):
        return array.astype(jnp.float32).reshape(length, heads, width)
    result_tokens = gated_scan(split_heads(probe_tokens, HEAD_K) * HEAD_K ** (-0.5), split_heads(lookup_tokens, HEAD_K), split_heads(content_tokens, HEAD_V), split_heads(forgetting_scores, HEAD_K))
    result_tokens = result_tokens * lax.rsqrt(lax.optimization_barrier(jnp.mean(result_tokens * result_tokens, axis=-1, keepdims=True)) + norm_eps)
    result_tokens = result_tokens * attend_unit_scale.astype(jnp.float32).reshape(heads, HEAD_V)
    switched_result = result_tokens.reshape(length, heads * HEAD_V) * jax.nn.silu(result_switch.astype(jnp.float32))
    return switched_result.astype(jnp.bfloat16)

def causal_conv(content_tokens, taps):
    content_tokens = content_tokens.astype(jnp.float32)
    taps = taps.astype(jnp.float32)
    width = taps.shape[0]
    padded = jnp.pad(content_tokens, ((width - 1, 0), (0, 0)))
    total = jnp.zeros_like(content_tokens)
    for offset in range(width):
        total = total + padded[offset:offset + content_tokens.shape[0]] * taps[offset]
    return total

def grouped_product(content_tokens, weight):
    group = content_tokens.shape[1] // N_TP
    total = jnp.zeros((content_tokens.shape[0], weight.shape[1]), jnp.float32)
    for index in range(N_TP):
        partial_sum = jnp.dot(content_tokens[:, index * group:(index + 1) * group], weight[index * group:(index + 1) * group], preferred_element_type=jnp.float32)
        total = total + lax.optimization_barrier(partial_sum.astype(jnp.bfloat16)).astype(jnp.float32)
    return total.astype(jnp.bfloat16)

def reference(incoming_features, attend_prenormal_scale, probe_matrix, lookup_matrix, content_matrix, forgetting_matrix, result_switch_matrix, forgetting_shift, spike_forget_logarithm, attend_unit_scale, attend_result_matrix, perceptron_scale, content_expand_matrix, switch_expand_matrix, content_kernel, switch_kernel, contract_matrix):

    def lone_context(incoming_tokens):
        weight_fragments, spike_forgetting = incoming_tokens
        normed = row_norm(weight_fragments, attend_prenormal_scale)
        probe_tokens = jnp.dot(normed, probe_matrix, preferred_element_type=jnp.float32).astype(jnp.bfloat16)
        lookup_tokens = jnp.dot(normed, lookup_matrix, preferred_element_type=jnp.float32).astype(jnp.bfloat16)
        content_tokens = jnp.dot(normed, content_matrix, preferred_element_type=jnp.float32).astype(jnp.bfloat16)
        result_switch = jnp.dot(normed, result_switch_matrix, preferred_element_type=jnp.float32).astype(jnp.bfloat16)
        forgetting_raw = jnp.dot(normed, forgetting_matrix, preferred_element_type=jnp.float32) + forgetting_shift
        switched_result = attend_unit_results(probe_tokens, lookup_tokens, content_tokens, result_switch, forgetting_raw, spike_forgetting, attend_unit_scale)
        mix = grouped_product(switched_result, attend_result_matrix)
        middle = (weight_fragments.astype(jnp.float32) + lax.optimization_barrier(mix).astype(jnp.float32)).astype(jnp.bfloat16)
        normed_mid = row_norm(middle, perceptron_scale)
        up_value = jnp.dot(normed_mid, content_expand_matrix, preferred_element_type=jnp.float32).astype(jnp.bfloat16)
        up_gate = jnp.dot(normed_mid, switch_expand_matrix, preferred_element_type=jnp.float32).astype(jnp.bfloat16)
        conv_value = causal_conv(up_value, content_kernel)
        conv_gated = causal_conv(up_gate, switch_kernel)
        hidden = (conv_value * jax.nn.gelu(conv_gated, approximate=True)).astype(jnp.bfloat16)
        ffn = grouped_product(hidden, contract_matrix)
        return (middle.astype(jnp.float32) + lax.optimization_barrier(ffn).astype(jnp.float32)).astype(jnp.bfloat16)
    result_tokens = lax.map(lone_context, (incoming_features.reshape(BATCH_SIZE, CONTEXT_SPAN, EMBED_DIM), spike_forget_logarithm.reshape(BATCH_SIZE, CONTEXT_SPAN, LOOKUP_FEATURES)))
    return result_tokens.reshape(TOKENS, EMBED_DIM)
```

```python
import functools
import heapq

import jax
import jax.numpy as jnp
from jax import lax
from jax.experimental import pallas as pl
from jax.experimental.pallas import tpu as pltpu
from jax.sharding import PartitionSpec as P

HEAD_K = 32
HEAD_V = 64
SUB = 16
NEVER = -1e30
norm_eps = 1e-06
MESH = pl.DeviceIdType.MESH
WIDTH = 2176
PARTS = (
    (0, "A", 0, 256),
    (0, "B", 256, 640),
    (1, "A", 640, 1280),
    (1, "B", 1280, 2176),
)
LENGTH = 192
GROUP = 8
COLS = 256
GELU = 0.7978845608028654

ROWS = 64
SIZES = {"y": 4, "z": 8}


def tree_messages(cls, tree, lo, hi):
    first, second = ("y", "z") if tree == "A" else ("z", "y")
    msgs = []

    def chain(axis, base, r0, rn, dep, stage):
        n = SIZES[axis]
        made = []
        for sign in (1, -1):
            d, s = dep, stage
            for k in range(1, n // 2 + 1):
                o = dict(base)
                o[axis] = sign * (k - 1)
                a0, an = r0, rn
                if k == n // 2:
                    an = rn // 2
                    a0 = r0 + (0 if sign > 0 else an)
                m = dict(cls=cls, lo=lo, hi=hi, axis=axis, sign=sign, o=o, r0=a0, rn=an, dep=d, stage=s, off=sign * k)
                msgs.append(m)
                made.append(m)
                d, s = m, s + 1
        return made

    made = chain(first, {"y": 0, "z": 0}, 0, ROWS, None, 0)
    chain(second, {"y": 0, "z": 0}, 0, ROWS, None, 0)
    for m in made:
        chain(second, {first: m["off"], second: 0}, m["r0"], m["rn"], m, m["stage"] + 1)
    return msgs


def plan(parts, rate=46.6e3, lat=1.9, ready=None):
    msgs = []
    for p in parts:
        msgs += tree_messages(*p)
    for i, m in enumerate(msgs):
        m["id"] = i
        m["bytes"] = m["rn"] * (m["hi"] - m["lo"]) * 2
    kids = {}
    for m in msgs:
        kids.setdefault(m["dep"]["id"] if m["dep"] else None, []).append(m)
    depth = {}
    def dep_depth(m):
        if m["id"] not in depth:
            depth[m["id"]] = 1 + max([dep_depth(k) for k in kids.get(m["id"], [])], default=0)
        return depth[m["id"]]
    free = {(a, s): 0.0 for a in "yz" for s in (1, -1)}
    avail = {k: [] for k in free}
    events = [(0.0, 0, m["id"]) for m in kids[None]]
    heapq.heapify(events)
    order = []
    t = 0.0
    pending = sorted(events)
    ev = list(pending)
    heapq.heapify(ev)
    n = 0
    while ev:
        t = ev[0][0]
        while ev and ev[0][0] <= t + 1e-9:
            _, kind, i = heapq.heappop(ev)
            if kind == 0:
                m = msgs[i]
                heapq.heappush(avail[(m["axis"], m["sign"])], (m["cls"], -dep_depth(m), i))
        for link, q in avail.items():
            if q and free[link] <= t + 1e-9:
                _, _, i = heapq.heappop(q)
                m = msgs[i]
                m["start"] = t
                free[link] = t + m["bytes"] / rate
                m["arrive"] = free[link] + lat
                order.append(m)
                heapq.heappush(ev, (free[link], 1, 0))
                for k in kids.get(i, []):
                    heapq.heappush(ev, (m["arrive"], 0, k["id"]))
    return order


def neighbour(axis, sign):
    rep, fs = lax.axis_index("rep"), lax.axis_index("fs")
    y, z = lax.rem(fs, 4), rep * 8 + fs // 4
    if axis == "y":
        y = lax.rem(y + 4 + sign, 4)
    else:
        z = lax.rem(z + 16 + sign, 16)
    return {"rep": z // 8, "fs": lax.rem(z, 8) * 4 + y}


def block_of(o):
    fs = lax.axis_index("fs")
    y, z = lax.rem(fs, 4), fs // 4
    y = lax.rem(y + 8 - o["y"], 4)
    z = lax.rem(z + 16 - o["z"], 8)
    return z * 4 + y


def attention_pieces(q, k, v, g, ld, unit, roll):
    length = q.shape[0]
    blocks = length // SUB
    exact = lax.Precision.HIGHEST
    row = lax.broadcasted_iota(jnp.int32, (length, 64), 0) % SUB
    c = ld
    shift = 1
    while shift < SUB:
        c = c + jnp.where(row >= shift, roll(c, shift), 0.0)
        shift *= 2
    key_head = lax.broadcasted_iota(jnp.int32, (64, 128), 0) // HEAD_K
    value_head = lax.broadcasted_iota(jnp.int32, (64, 128), 1) // HEAD_V
    spread = jnp.where(key_head == value_head, 1.0, 0.0)
    c3 = c.reshape(blocks, SUB, 64)
    total = c3[:, SUB - 1 : SUB, :]
    k_end = (k.reshape(blocks, SUB, 64) * jnp.exp(total - c3))
    q_in = q * jnp.exp(c)
    v3 = v.reshape(blocks, SUB, 128)
    fade = jnp.exp(total)
    q3 = q_in.reshape(blocks, SUB, 64)
    own_head = (
        lax.broadcasted_iota(jnp.int32, (128, 64), 0) // HEAD_V
        == lax.broadcasted_iota(jnp.int32, (128, 64), 1) // HEAD_K
    )
    yield None
    out = jnp.zeros((length, 128), jnp.float32)
    for j in range(SUB):
        if j == 0:
            pairs, values = q * k, v
        else:
            differ = jnp.where(row >= j, c - roll(c, j), NEVER)
            pairs, values = q * roll(k, j) * jnp.exp(differ), roll(v, j)
        scores = jnp.dot(pairs, spread, precision=exact, preferred_element_type=jnp.float32)
        out = out + scores * values
        if j % 4 == 3:
            yield None
    state = None
    carried = [jnp.zeros((SUB, 128), jnp.float32)]
    for i in range(blocks):
        if state is not None:
            carried.append(
                lax.dot_general(
                    q3[i], state, (((1,), (1,)), ((), ())), precision=exact,
                    preferred_element_type=jnp.float32,
                )
            )
        if i < blocks - 1:
            update = lax.dot_general(
                v3[i], k_end[i], (((0,), (0,)), ((), ())), precision=exact,
                preferred_element_type=jnp.float32,
            )
            update = jnp.where(own_head, update, 0.0)
            state = update if state is None else state * fade[i] + update
        if i % 4 == 3:
            yield None
    out = out + jnp.concatenate(carried, axis=0)
    same = jnp.where(
        lax.broadcasted_iota(jnp.int32, (128, 128), 0) // HEAD_V
        == lax.broadcasted_iota(jnp.int32, (128, 128), 1) // HEAD_V,
        1.0 / HEAD_V,
        0.0,
    )
    mean = jnp.dot(out * out, same, precision=exact, preferred_element_type=jnp.float32)
    out = out * lax.rsqrt(mean + norm_eps) * unit * (g / (1.0 + jnp.exp(-g)))
    yield out.astype(jnp.bfloat16)


def rows_norm(blocks, gain_ref, out):
    total = jnp.zeros((LENGTH, COLS), jnp.float32)
    for t in range(GROUP):
        one = blocks[t].astype(jnp.float32)
        total = total + one * one
    mean = jnp.sum(total, axis=1, keepdims=True) * (1.0 / (GROUP * COLS))
    scale = lax.rsqrt(mean + norm_eps)
    for t in range(GROUP):
        at = slice(t * COLS, (t + 1) * COLS)
        gain = gain_ref[:, at].astype(jnp.float32)
        out[:, at] = (blocks[t].astype(jnp.float32) * scale * gain).astype(jnp.bfloat16)


def short_conv(tokens, taps):
    row = lax.broadcasted_iota(jnp.int32, tokens.shape, 0)
    one = jnp.where(row >= 1, pltpu.roll(tokens, 1, 0), 0.0)
    two = jnp.where(row >= 2, pltpu.roll(tokens, 2, 0), 0.0)
    return two * taps[0:1] + one * taps[1:2] + tokens * taps[2:3]


def layer_kernel(
    order,
    packed_ref,
    x_ref,
    pre_ref,
    shift_ref,
    spike_ref,
    unit_ref,
    post_ref,
    value_taps,
    gate_taps,
    out_ref,
    whole,
    x_all,
    mid_all,
    sums,
    from_partner,
    pair_sums,
    from_chips,
    down_from_partner,
    down_pair_sums,
    down_from_chips,
    normed,
    hidden,
    own_sem,
    send_sem,
    recv_sem,
    tp_send,
    tp_recv,
):
    f32, bf16 = jnp.float32, jnp.bfloat16
    tp = lax.axis_index("tp")
    chip, core = tp // 2, lax.rem(tp, 2)
    partner = chip * 2 + (1 - core)

    def peer(d):
        return lax.rem(chip + 4 + d, 4) * 2 + core

    barrier = pltpu.get_barrier_semaphore()
    for axis in ("y", "z"):
        for sign in (1, -1):
            pl.semaphore_signal(
                barrier, inc=1, device_id=neighbour(axis, sign), device_id_type=MESH
            )
    for other in (peer(1), peer(2), peer(3), partner):
        pl.semaphore_signal(barrier, inc=1, device_id={"tp": other}, device_id_type=MESH)
    mine = pl.multiple_of(lax.axis_index("fs") * ROWS, ROWS)
    own = [
        pltpu.make_async_copy(packed_ref, whole.at[pl.ds(mine, ROWS)], own_sem.at[0]),
        pltpu.make_async_copy(x_ref, x_all.at[tp], own_sem.at[1]),
    ]
    for one in own:
        one.start()
    for one in own:
        one.wait()
    pl.semaphore_wait(barrier, 8)

    def copy_of(m, step):
        o = dict(m["o"])
        o[m["axis"]] = o[m["axis"]] + step * m["sign"]
        row = pl.multiple_of(block_of(o) * ROWS + m["r0"], 16)
        at = whole.at[pl.ds(row, m["rn"]), pl.ds(m["lo"], m["hi"] - m["lo"])]
        return pltpu.make_async_remote_copy(
            src_ref=at,
            dst_ref=at,
            send_sem=send_sem.at[m["id"]],
            recv_sem=recv_sem.at[m["id"]],
            device_id=neighbour(m["axis"], m["sign"]),
            device_id_type=MESH,
        )

    seen, at_message = set(), [0]

    def arrived(m):
        if m["id"] not in seen:
            copy_of(m, 1).wait_recv()
            seen.add(m["id"])

    def pump(until):
        while at_message[0] < len(order) and order[at_message[0]]["start"] <= until:
            m = order[at_message[0]]
            if m["dep"] is not None:
                arrived(m["dep"])
            copy_of(m, 0).start()
            at_message[0] += 1

    def class_arrived(cls):
        mine_of = sorted((m for m in order if m["cls"] == cls), key=lambda m: m["arrive"])
        for m in mine_of:
            pump(m["arrive"])
            arrived(m)
        return mine_of[-1]["arrive"]

    def tp_copy(src, dst, number, to):
        return pltpu.make_async_remote_copy(
            src_ref=src,
            dst_ref=dst,
            send_sem=tp_send.at[number],
            recv_sem=tp_recv.at[number],
            device_id={"tp": to},
            device_id_type=MESH,
        )

    started = []

    def begin(copy):
        copy.start()
        started.append(copy)

    def share(buf, base):
        for d in (2, 1, 3):
            begin(tp_copy(buf.at[tp], buf.at[tp], base + d - 1, peer(d)))
        begin(tp_copy(buf.at[tp], buf.at[tp], base + 3, partner))

    def share_on(buf, base):
        for d in (1, 3, 2):
            came = buf.at[peer(-d)]
            tp_copy(came, came, base + d - 1, peer(d)).wait_recv()
            begin(tp_copy(came, came, base + 3 + d, partner))

    def shared(buf, base):
        for d in range(4):
            came = buf.at[lax.rem(chip + 4 - d, 4) * 2 + (1 - core)]
            tp_copy(came, came, base + 3 + d, partner).wait_recv()

    def summed(product, got, paired, chips, base, clock):
        waiting = []
        for d in (2, 1, 3, 0):
            there = lax.rem(chip + d, 4) * 2
            for who in (1 - core, core):
                sums[there + who] = product(there + who).astype(bf16)
            for copy in waiting:
                begin(copy)
            waiting = [tp_copy(sums.at[there + 1 - core], got.at[d], base + d, partner)]
            pump(clock(d))
        for copy in waiting:
            begin(copy)
        waiting = []
        for d in (2, 1, 3):
            there = lax.rem(chip + d, 4) * 2 + core
            tp_copy(sums.at[there], got.at[d], base + d, partner).wait_recv()
            paired[d - 1] = (sums[there].astype(f32) + got[d].astype(f32)).astype(bf16)
            for copy in waiting:
                begin(copy)
            waiting = [tp_copy(paired.at[d - 1], chips.at[d - 1], base + 3 + d, peer(d))]
        tp_copy(sums.at[tp], got.at[0], base, partner).wait_recv()
        for copy in waiting:
            begin(copy)
        total = sums[tp].astype(f32) + got[0].astype(f32)
        return total

    def chips_added(total, chips, base):
        for d in (1, 3, 2):
            tp_copy(chips.at[d - 1], chips.at[d - 1], base + 3 + d, peer(d)).wait_recv()
            total = total + chips[d - 1].astype(f32)
        return total

    last = order[-1]["start"]
    share(x_all, 0)
    pump(T_SHARE)
    share_on(x_all, 0)
    pump(T_SHARED)
    shared(x_all, 0)
    rows_norm(x_all, pre_ref, normed)
    now = class_arrived(0)

    first = jnp.dot(normed[...], whole[:, 0:256], preferred_element_type=f32)
    second = jnp.dot(normed[...], whole[:, 256:512], preferred_element_type=f32)
    pump(now + 2.0)
    rounded = first.astype(bf16).astype(f32)
    query = rounded[:, 0:64] * HEAD_K ** (-0.5)
    key = rounded[:, 64:128]
    value = rounded[:, 128:256]
    gate = second[:, 0:128].astype(bf16).astype(f32)
    forget = second[:, 128:192] + shift_ref[...]
    decay = -(jnp.maximum(-forget, 0.0) + jnp.log1p(jnp.exp(-jnp.abs(forget)))) / 16.0
    decay = decay + spike_ref[...]
    unit = unit_ref[...].astype(f32)
    now = now + 2.0
    for piece in attention_pieces(
        query, key, value, gate, decay, unit, lambda a, s: pltpu.roll(a, s, 0)
    ):
        now = now + T_PIECE
        pump(now)
        gated = piece

    def mix_part(t):
        rows = pl.ds(pl.multiple_of(t * COLS, COLS), COLS)
        return lax.dot_general(
            gated, whole[rows, 512:640], (((1,), (1,)), ((), ())), preferred_element_type=f32
        )

    begun = now
    total = summed(mix_part, from_partner, pair_sums, from_chips, 8, lambda d: begun + 2.0)
    pump(begun + 5.0)
    mix = chips_added(total, from_chips, 8).astype(bf16)
    mid_all[tp] = (x_all[tp].astype(f32) + mix.astype(f32)).astype(bf16)
    pump(begun + 9.0)
    share(mid_all, 16)
    pump(begun + 12.0)
    share_on(mid_all, 16)
    pump(begun + 15.0)
    shared(mid_all, 16)
    rows_norm(mid_all, post_ref, normed)
    pump(last)
    class_arrived(1)

    for block in range(4):
        at = block * 128
        cols = slice(at, at + 128)
        up_value = jnp.dot(
            normed[...], whole[:, 640 + at : 768 + at], preferred_element_type=f32
        )
        up_gate = jnp.dot(
            normed[...], whole[:, 1152 + at : 1280 + at], preferred_element_type=f32
        )
        conv_value = short_conv(up_value.astype(bf16).astype(f32), value_taps[:, cols].astype(f32))
        conv_gate = short_conv(up_gate.astype(bf16).astype(f32), gate_taps[:, cols].astype(f32))
        cube = conv_gate + 0.044715 * (conv_gate * conv_gate * conv_gate)
        gelu = conv_gate * (0.5 * (1.0 + jnp.tanh(GELU * cube)))
        hidden[:, cols] = (conv_value * gelu).astype(bf16)

    def down_part(t):
        rows = pl.ds(pl.multiple_of(t * COLS, COLS), COLS)
        return lax.dot_general(
            hidden[...], whole[rows, 1664:2176], (((1,), (1,)), ((), ())), preferred_element_type=f32
        )

    for copy in started[7:14]:
        copy.wait_send()
    total = summed(down_part, down_from_partner, down_pair_sums, down_from_chips, 24, lambda d: last)
    ffn = chips_added(total, down_from_chips, 24).astype(bf16)
    out_ref[...] = (mid_all[tp].astype(f32) + ffn.astype(f32)).astype(bf16)

    for copy in started[:7] + started[14:]:
        copy.wait_send()
    for m in order:
        copy_of(m, 0).wait_send()


T_SHARE = 4.0
T_SHARED = 9.0
T_PIECE = 0.7


def shards(
    incoming_features,
    attend_prenormal_scale,
    probe_matrix,
    lookup_matrix,
    content_matrix,
    forgetting_matrix,
    result_switch_matrix,
    forgetting_shift,
    spike_forget_logarithm,
    attend_unit_scale,
    attend_result_matrix,
    perceptron_scale,
    content_expand_matrix,
    switch_expand_matrix,
    content_kernel,
    switch_kernel,
    contract_matrix,
):
    packed = jnp.concatenate(
        (
            probe_matrix,
            lookup_matrix,
            content_matrix,
            result_switch_matrix,
            forgetting_matrix,
            jnp.zeros_like(forgetting_matrix),
            attend_result_matrix.T,
            content_expand_matrix,
            switch_expand_matrix,
            contract_matrix.T,
        ),
        axis=1,
    )
    order = plan(PARTS, rate=42e3, lat=2.5)
    count = len(order)
    block = (LENGTH, COLS)
    dma = pltpu.SemaphoreType.DMA
    vmem = pl.BlockSpec(memory_space=pltpu.VMEM)
    hbm = pl.BlockSpec(memory_space=pl.ANY)
    bf16 = jnp.bfloat16
    return pl.pallas_call(
        functools.partial(layer_kernel, order),
        out_shape=jax.ShapeDtypeStruct(block, bf16),
        in_specs=[hbm, hbm] + [vmem] * 7,
        out_specs=vmem,
        scratch_shapes=[
            pltpu.VMEM((32 * ROWS, WIDTH), bf16),
            pltpu.VMEM((GROUP, *block), bf16),
            pltpu.VMEM((GROUP, *block), bf16),
            pltpu.VMEM((GROUP, *block), bf16),
            pltpu.VMEM((4, *block), bf16),
            pltpu.VMEM((3, *block), bf16),
            pltpu.VMEM((3, *block), bf16),
            pltpu.VMEM((4, *block), bf16),
            pltpu.VMEM((3, *block), bf16),
            pltpu.VMEM((3, *block), bf16),
            pltpu.VMEM((LENGTH, GROUP * COLS), bf16),
            pltpu.VMEM((LENGTH, 512), bf16),
            dma((2,)),
            dma((count,)),
            dma((count,)),
            dma((32,)),
            dma((32,)),
        ],
        compiler_params=pltpu.CompilerParams(
            collective_id=0, has_side_effects=True, vmem_limit_bytes=48 * 1024 * 1024
        ),
    )(
        packed,
        incoming_features,
        attend_prenormal_scale[None],
        forgetting_shift[None],
        spike_forget_logarithm,
        attend_unit_scale[None],
        perceptron_scale[None],
        content_kernel,
        switch_kernel,
    )


def solution(mesh):
    placed = (
        P(("rep", "fs"), "tp"),
        P(),
        P("fs", "tp"),
        P("fs", "tp"),
        P("fs", "tp"),
        P("fs", "tp"),
        P("fs", "tp"),
        P("tp"),
        P(("rep", "fs"), "tp"),
        P("tp"),
        P("tp", "fs"),
        P(),
        P("fs", "tp"),
        P("fs", "tp"),
        P(None, "tp"),
        P(None, "tp"),
        P("tp", "fs"),
    )
    return jax.shard_map(
        shards, mesh=mesh, in_specs=placed, out_specs=P(("rep", "fs"), "tp"), check_vma=False
    )
```

```python
import functools
import heapq

import jax
import jax.numpy as jnp
from jax import lax
from jax.experimental import pallas as pl
from jax.experimental.pallas import tpu as pltpu
from jax.sharding import PartitionSpec as P

HEAD_K = 32
HEAD_V = 64
SUB = 16
NEVER = -1e30
norm_eps = 1e-06
MESH = pl.DeviceIdType.MESH
WIDTH = 2176
PARTS = (
    (0, "A", 0, 256),
    (0, "B", 256, 640),
    (1, "A", 640, 1280),
    (1, "B", 1280, 2176),
)
LENGTH = 192
GROUP = 8
COLS = 256
GELU = 0.7978845608028654

ROWS = 64
SIZES = {"y": 4, "z": 8}


def tree_messages(cls, tree, lo, hi):
    first, second = ("y", "z") if tree == "A" else ("z", "y")
    msgs = []

    def chain(axis, base, deps, stage):
        n = SIZES[axis]
        made = []
        for sign in (1, -1):
            d, s = deps, stage
            for k in range(1, n // 2 + 1):
                o = dict(base)
                o[axis] = sign * (k - 1)
                r0, rn = 0, ROWS
                if k == n // 2:
                    rn = ROWS // 2
                    r0 = 0 if sign > 0 else rn
                m = dict(
                    cls=cls, lo=lo, hi=hi, axis=axis, sign=sign, o=o, r0=r0, rn=rn, deps=d, off=sign * k, stage=s
                )
                msgs.append(m)
                made.append(m)
                d, s = (m,), s + 1
        return made

    made = chain(first, {"y": 0, "z": 0}, (), 0)
    chain(second, {"y": 0, "z": 0}, (), 0)
    far = SIZES[first] // 2
    for m in made:
        if abs(m["off"]) < far:
            chain(second, {first: m["off"], second: 0}, (m,), m["stage"] + 1)
    halves = tuple(m for m in made if abs(m["off"]) == far)
    chain(second, {first: far, second: 0}, halves, halves[0]["stage"] + 1)
    return msgs


def plan(parts, rate, lat, each):
    msgs = []
    for p in parts:
        msgs += tree_messages(*p)
    kids = {}
    for i, m in enumerate(msgs):
        m["id"] = i
        m["bytes"] = m["rn"] * (m["hi"] - m["lo"]) * 2
        m["need"] = len(m["deps"])
        for d in m["deps"]:
            kids.setdefault(d["id"], []).append(m)
    depth = {}

    def depth_of(m):
        if m["id"] not in depth:
            depth[m["id"]] = 1 + max((depth_of(k) for k in kids.get(m["id"], ())), default=0)
        return depth[m["id"]]

    free = {(a, s): 0.0 for a in "yz" for s in (1, -1)}
    avail = {k: [] for k in free}
    events = [(0.0, 0, m["id"]) for m in msgs if not m["deps"]]
    heapq.heapify(events)
    order = []
    while events:
        t = events[0][0]
        while events and events[0][0] <= t + 1e-9:
            _, kind, i = heapq.heappop(events)
            if kind == 0:
                m = msgs[i]
                heapq.heappush(avail[(m["axis"], m["sign"])], (m["cls"], -depth_of(m), i))
        for link, queue in avail.items():
            if queue and free[link] <= t + 1e-9:
                m = msgs[heapq.heappop(queue)[2]]
                m["start"] = t
                free[link] = t + m["bytes"] / rate + each
                m["arrive"] = free[link] + lat
                order.append(m)
                heapq.heappush(events, (free[link], 1, 0))
                for k in kids.get(m["id"], ()):
                    k["need"] -= 1
                    if k["need"] == 0:
                        heapq.heappush(events, (m["arrive"], 0, k["id"]))
    return order


def neighbour(axis, sign):
    rep, fs = lax.axis_index("rep"), lax.axis_index("fs")
    y, z = lax.rem(fs, 4), rep * 8 + fs // 4
    if axis == "y":
        y = lax.rem(y + 4 + sign, 4)
    else:
        z = lax.rem(z + 16 + sign, 16)
    return {"rep": z // 8, "fs": lax.rem(z, 8) * 4 + y}


def block_of(o):
    fs = lax.axis_index("fs")
    y, z = lax.rem(fs, 4), fs // 4
    y = lax.rem(y + 8 - o["y"], 4)
    z = lax.rem(z + 16 - o["z"], 8)
    return z * 4 + y


def attention_pieces(q, k, v, g, ld, unit, roll):
    length = q.shape[0]
    blocks = length // SUB
    exact = lax.Precision.HIGHEST
    row = lax.broadcasted_iota(jnp.int32, (length, 64), 0) % SUB
    c = ld
    shift = 1
    while shift < SUB:
        c = c + jnp.where(row >= shift, roll(c, shift), 0.0)
        shift *= 2
    key_head = lax.broadcasted_iota(jnp.int32, (64, 128), 0) // HEAD_K
    value_head = lax.broadcasted_iota(jnp.int32, (64, 128), 1) // HEAD_V
    spread = jnp.where(key_head == value_head, 1.0, 0.0)
    c3 = c.reshape(blocks, SUB, 64)
    total = c3[:, SUB - 1 : SUB, :]
    k_end = (k.reshape(blocks, SUB, 64) * jnp.exp(total - c3))
    q_in = q * jnp.exp(c)
    v3 = v.reshape(blocks, SUB, 128)
    fade = jnp.exp(total)
    q3 = q_in.reshape(blocks, SUB, 64)
    own_head = (
        lax.broadcasted_iota(jnp.int32, (128, 64), 0) // HEAD_V
        == lax.broadcasted_iota(jnp.int32, (128, 64), 1) // HEAD_K
    )
    yield None
    out = jnp.zeros((length, 128), jnp.float32)
    for j in range(SUB):
        if j == 0:
            pairs, values = q * k, v
        else:
            differ = jnp.where(row >= j, c - roll(c, j), NEVER)
            pairs, values = q * roll(k, j) * jnp.exp(differ), roll(v, j)
        scores = jnp.dot(pairs, spread, precision=exact, preferred_element_type=jnp.float32)
        out = out + scores * values
        if j % 4 == 3:
            yield None
    state = None
    carried = [jnp.zeros((SUB, 128), jnp.float32)]
    for i in range(blocks):
        if state is not None:
            carried.append(
                lax.dot_general(
                    q3[i], state, (((1,), (1,)), ((), ())), precision=exact,
                    preferred_element_type=jnp.float32,
                )
            )
        if i < blocks - 1:
            update = lax.dot_general(
                v3[i], k_end[i], (((0,), (0,)), ((), ())), precision=exact,
                preferred_element_type=jnp.float32,
            )
            update = jnp.where(own_head, update, 0.0)
            state = update if state is None else state * fade[i] + update
        if i % 4 == 3:
            yield None
    out = out + jnp.concatenate(carried, axis=0)
    same = jnp.where(
        lax.broadcasted_iota(jnp.int32, (128, 128), 0) // HEAD_V
        == lax.broadcasted_iota(jnp.int32, (128, 128), 1) // HEAD_V,
        1.0 / HEAD_V,
        0.0,
    )
    mean = jnp.dot(out * out, same, precision=exact, preferred_element_type=jnp.float32)
    out = out * lax.rsqrt(mean + norm_eps) * unit * (g / (1.0 + jnp.exp(-g)))
    yield out.astype(jnp.bfloat16)


def rows_norm(blocks, gain_ref, which, out):
    total = jnp.zeros((LENGTH, COLS), jnp.float32)
    for t in range(GROUP):
        one = blocks[t].astype(jnp.float32)
        total = total + one * one
    mean = jnp.sum(total, axis=1, keepdims=True) * (1.0 / (GROUP * COLS))
    scale = lax.rsqrt(mean + norm_eps)
    for t in range(GROUP):
        at = slice(t * COLS, (t + 1) * COLS)
        gain = gain_ref[which : which + 1, at].astype(jnp.float32)
        out[:, at] = (blocks[t].astype(jnp.float32) * scale * gain).astype(jnp.bfloat16)


def short_conv(tokens, taps):
    row = lax.broadcasted_iota(jnp.int32, tokens.shape, 0)
    one = jnp.where(row >= 1, pltpu.roll(tokens, 1, 0), 0.0)
    two = jnp.where(row >= 2, pltpu.roll(tokens, 2, 0), 0.0)
    return two * taps[0:1] + one * taps[1:2] + tokens * taps[2:3]


def layer_kernel(
    order,
    packed_ref,
    value_ref,
    gate_ref,
    down_ref,
    x_ref,
    gains_ref,
    shift_ref,
    spike_ref,
    unit_ref,
    value_taps,
    gate_taps,
    out_ref,
    whole,
    x_all,
    mid_all,
    sums,
    from_partner,
    pair_sums,
    passing,
    passed,
    from_chips,
    down_from_partner,
    down_pair_sums,
    down_passing,
    down_passed,
    down_from_chips,
    normed,
    hidden,
    own_sem,
    send_sem,
    recv_sem,
    tp_send,
    tp_recv,
):
    f32, bf16 = jnp.float32, jnp.bfloat16
    tp = lax.axis_index("tp")
    chip, core = tp // 2, lax.rem(tp, 2)
    partner = chip * 2 + (1 - core)

    def peer(d):
        return lax.rem(chip + 4 + d, 4) * 2 + core

    barrier = pltpu.get_barrier_semaphore()
    for axis in ("y", "z"):
        for sign in (1, -1):
            pl.semaphore_signal(
                barrier, inc=1, device_id=neighbour(axis, sign), device_id_type=MESH
            )
    for other in (peer(1), peer(3), partner):
        pl.semaphore_signal(barrier, inc=1, device_id={"tp": other}, device_id_type=MESH)
    mine = pl.ds(pl.multiple_of(lax.axis_index("fs") * ROWS, ROWS), ROWS)
    own = [
        pltpu.make_async_copy(packed_ref, whole.at[mine, pl.ds(0, 640)], own_sem.at[0]),
        pltpu.make_async_copy(value_ref, whole.at[mine, pl.ds(640, 512)], own_sem.at[1]),
        pltpu.make_async_copy(gate_ref, whole.at[mine, pl.ds(1152, 512)], own_sem.at[2]),
        pltpu.make_async_copy(down_ref, whole.at[mine, pl.ds(1664, 512)], own_sem.at[3]),
        pltpu.make_async_copy(x_ref, x_all.at[tp], own_sem.at[4]),
    ]
    for one in own:
        one.start()
    for one in own:
        one.wait()
    pl.semaphore_wait(barrier, 7)

    def copy_of(m, step):
        o = dict(m["o"])
        o[m["axis"]] = o[m["axis"]] + step * m["sign"]
        row = pl.multiple_of(block_of(o) * ROWS + m["r0"], 16)
        at = whole.at[pl.ds(row, m["rn"]), pl.ds(m["lo"], m["hi"] - m["lo"])]
        return pltpu.make_async_remote_copy(
            src_ref=at,
            dst_ref=at,
            send_sem=send_sem.at[0],
            recv_sem=recv_sem.at[m["id"]],
            device_id=neighbour(m["axis"], m["sign"]),
            device_id_type=MESH,
        )

    seen, at_message = set(), [0]

    def arrived(m):
        if m["id"] not in seen:
            copy_of(m, 1).wait_recv()
            seen.add(m["id"])

    def pump(until):
        while at_message[0] < len(order) and order[at_message[0]]["start"] <= until:
            m = order[at_message[0]]
            for d in m["deps"]:
                arrived(d)
            copy_of(m, 0).start()
            at_message[0] += 1

    def class_arrived(cls):
        mine_of = sorted((m for m in order if m["cls"] == cls), key=lambda m: m["arrive"])
        for m in mine_of:
            pump(m["arrive"])
            arrived(m)
        return mine_of[-1]["arrive"]

    def tp_copy(src, dst, number, to):
        return pltpu.make_async_remote_copy(
            src_ref=src,
            dst_ref=dst,
            send_sem=tp_send.at[number],
            recv_sem=tp_recv.at[number],
            device_id={"tp": to},
            device_id_type=MESH,
        )

    started = []

    def begin(copy):
        copy.start()
        started.append(copy)

    right, left = peer(1), peer(3)
    low, high = pl.ds(0, LENGTH // 2), pl.ds(LENGTH // 2, LENGTH // 2)

    def move(buf, owner, rows, number, to):
        at = buf.at[owner, rows]
        return tp_copy(at, at, number, to)

    def share(buf, base):
        begin(move(buf, tp, low, base, right))
        begin(move(buf, tp, high, base + 1, left))
        begin(move(buf, tp, high, base + 2, right))
        begin(move(buf, tp, low, base + 3, left))
        begin(tp_copy(buf.at[tp], buf.at[tp], base + 6, partner))

    def share_on(buf, base):
        move(buf, left, low, base, right).wait_recv()
        begin(move(buf, left, low, base + 4, right))
        move(buf, right, high, base + 1, left).wait_recv()
        begin(move(buf, right, high, base + 5, left))
        move(buf, left, high, base + 2, right).wait_recv()
        begin(tp_copy(buf.at[left], buf.at[left], base + 7, partner))
        move(buf, right, low, base + 3, left).wait_recv()
        begin(tp_copy(buf.at[right], buf.at[right], base + 8, partner))

    def shared(buf, base):
        far = peer(2)
        move(buf, far, low, base + 4, right).wait_recv()
        move(buf, far, high, base + 5, left).wait_recv()
        begin(tp_copy(buf.at[far], buf.at[far], base + 9, partner))
        for k, d in enumerate((0, 3, 1, 2)):
            came = buf.at[lax.rem(chip + d, 4) * 2 + (1 - core)]
            tp_copy(came, came, base + 6 + k, partner).wait_recv()

    def summed(product, got, paired, through, joined, chips, base, clock):
        waiting = []
        for d in (2, 1, 3, 0):
            there = lax.rem(chip + d, 4) * 2
            for who in (1 - core, core):
                sums[there + who] = product(there + who).astype(bf16)
            for copy in waiting:
                begin(copy)
            waiting = [tp_copy(sums.at[there + 1 - core], got.at[d], base + d, partner)]
        for copy in waiting:
            begin(copy)
        for d in (2, 1, 3):
            there = lax.rem(chip + d, 4) * 2 + core
            tp_copy(sums.at[there], got.at[d], base + d, partner).wait_recv()
            paired[d - 1] = (sums[there].astype(f32) + got[d].astype(f32)).astype(bf16)
            if d == 1:
                begin(tp_copy(paired.at[1, low], through.at[0], base + 4, right))
                begin(tp_copy(paired.at[1, high], through.at[1], base + 5, left))
            if d == 3:
                begin(tp_copy(paired.at[0, high], chips.at[0, high], base + 6, right))
        tp_copy(sums.at[tp], got.at[0], base, partner).wait_recv()
        total = sums[tp].astype(f32) + got[0].astype(f32)
        begin(tp_copy(paired.at[2, low], chips.at[1, low], base + 7, left))
        clock()
        tp_copy(through.at[0], through.at[0], base + 4, right).wait_recv()
        half = LENGTH // 2
        joined[0] = (paired[0, 0:half].astype(f32) + through[0].astype(f32)).astype(bf16)
        tp_copy(through.at[1], through.at[1], base + 5, left).wait_recv()
        joined[1] = (paired[2, half:].astype(f32) + through[1].astype(f32)).astype(bf16)
        begin(tp_copy(joined.at[0], chips.at[0, low], base + 8, right))
        for copy in started[: len(started) - 9]:
            if id(copy) not in sent:
                sent.add(id(copy))
                copy.wait_send()
        begin(tp_copy(joined.at[1], chips.at[1, high], base + 9, left))
        clock()
        tp_copy(chips.at[0, high], chips.at[0, high], base + 6, right).wait_recv()
        tp_copy(chips.at[1, low], chips.at[1, low], base + 7, left).wait_recv()
        tp_copy(chips.at[0, low], chips.at[0, low], base + 8, right).wait_recv()
        tp_copy(chips.at[1, high], chips.at[1, high], base + 9, left).wait_recv()
        return total + chips[0].astype(f32) + chips[1].astype(f32)

    sent = set()
    share(x_all, 0)
    pump(T_SHARE)
    share_on(x_all, 0)
    pump(T_SHARED)
    shared(x_all, 0)
    rows_norm(x_all, gains_ref, 0, normed)
    now = class_arrived(0)

    first = jnp.dot(normed[...], whole[:, 0:256], preferred_element_type=f32)
    second = jnp.dot(normed[...], whole[:, 256:512], preferred_element_type=f32)
    pump(now + 2.0)
    rounded = first.astype(bf16).astype(f32)
    query = rounded[:, 0:64] * HEAD_K ** (-0.5)
    key = rounded[:, 64:128]
    value = rounded[:, 128:256]
    gate = second[:, 0:128].astype(bf16).astype(f32)
    forget = second[:, 128:192] + shift_ref[...]
    decay = -(jnp.maximum(-forget, 0.0) + jnp.log1p(jnp.exp(-jnp.abs(forget)))) / 16.0
    decay = decay + spike_ref[...]
    unit = unit_ref[...].astype(f32)
    now = now + 2.0
    for piece in attention_pieces(
        query, key, value, gate, decay, unit, lambda a, s: pltpu.roll(a, s, 0)
    ):
        now = now + T_PIECE
        pump(now)
        gated = piece

    def mix_part(t):
        rows = pl.ds(pl.multiple_of(t * COLS, COLS), COLS)
        return lax.dot_general(
            gated, whole[rows, 512:640], (((1,), (1,)), ((), ())), preferred_element_type=f32
        )

    ticks = [now]

    def tick(step):
        ticks[0] = ticks[0] + step
        pump(ticks[0])

    total = summed(
        mix_part, from_partner, pair_sums, passing, passed, from_chips, 10, lambda: tick(T_SUM)
    )
    mix = total.astype(bf16)
    mid_all[tp] = (x_all[tp].astype(f32) + mix.astype(f32)).astype(bf16)
    tick(T_MID)
    share(mid_all, 20)
    tick(T_MID)
    share_on(mid_all, 20)
    tick(T_MID)
    shared(mid_all, 20)
    rows_norm(mid_all, gains_ref, 1, normed)
    class_arrived(1)

    for block in range(4):
        at = block * 128
        cols = slice(at, at + 128)
        up_value = jnp.dot(
            normed[...], whole[:, 640 + at : 768 + at], preferred_element_type=f32
        )
        up_gate = jnp.dot(
            normed[...], whole[:, 1152 + at : 1280 + at], preferred_element_type=f32
        )
        conv_value = short_conv(up_value.astype(bf16).astype(f32), value_taps[:, cols].astype(f32))
        conv_gate = short_conv(up_gate.astype(bf16).astype(f32), gate_taps[:, cols].astype(f32))
        cube = conv_gate + 0.044715 * (conv_gate * conv_gate * conv_gate)
        gelu = conv_gate * (0.5 * (1.0 + jnp.tanh(GELU * cube)))
        hidden[:, cols] = (conv_value * gelu).astype(bf16)

    def down_part(t):
        rows = pl.ds(pl.multiple_of(t * COLS, COLS), COLS)
        return lax.dot_general(
            hidden[...], whole[rows, 1664:2176], (((1,), (1,)), ((), ())), preferred_element_type=f32
        )

    for copy in started:
        if id(copy) not in sent:
            sent.add(id(copy))
            copy.wait_send()
    total = summed(
        down_part,
        down_from_partner,
        down_pair_sums,
        down_passing,
        down_passed,
        down_from_chips,
        30,
        lambda: None,
    )
    out_ref[...] = (mid_all[tp].astype(f32) + total.astype(bf16).astype(f32)).astype(bf16)

    for copy in started:
        if id(copy) not in sent:
            copy.wait_send()
    rest = whole.at[pl.ds(0, 31 * ROWS)]
    pltpu.make_async_remote_copy(
        src_ref=rest,
        dst_ref=rest,
        send_sem=send_sem.at[0],
        recv_sem=recv_sem.at[0],
        device_id=neighbour("y", 1),
        device_id_type=MESH,
    ).wait_send()


T_SHARE = 4.0
T_SHARED = 9.0
T_PIECE = 0.7
T_SUM = 2.0
T_MID = 2.5


def shards(
    incoming_features,
    attend_prenormal_scale,
    probe_matrix,
    lookup_matrix,
    content_matrix,
    forgetting_matrix,
    result_switch_matrix,
    forgetting_shift,
    spike_forget_logarithm,
    attend_unit_scale,
    attend_result_matrix,
    perceptron_scale,
    content_expand_matrix,
    switch_expand_matrix,
    content_kernel,
    switch_kernel,
    contract_matrix,
):
    packed = jnp.concatenate(
        (
            probe_matrix,
            lookup_matrix,
            content_matrix,
            result_switch_matrix,
            forgetting_matrix,
            jnp.zeros_like(forgetting_matrix),
            attend_result_matrix.T,
        ),
        axis=1,
    )
    order = plan(PARTS, 44e3, 2.3, 0.07)
    count = len(order)
    block = (LENGTH, COLS)
    dma = pltpu.SemaphoreType.DMA
    vmem = pl.BlockSpec(memory_space=pltpu.VMEM)
    hbm = pl.BlockSpec(memory_space=pl.ANY)
    bf16 = jnp.bfloat16
    return pl.pallas_call(
        functools.partial(layer_kernel, order),
        out_shape=jax.ShapeDtypeStruct(block, bf16),
        in_specs=[hbm] * 5 + [vmem] * 6,
        out_specs=vmem,
        scratch_shapes=[
            pltpu.VMEM((32 * ROWS, WIDTH), bf16),
            pltpu.VMEM((GROUP, *block), bf16),
            pltpu.VMEM((GROUP, *block), bf16),
            pltpu.VMEM((GROUP, *block), bf16),
            pltpu.VMEM((4, *block), bf16),
            pltpu.VMEM((3, *block), bf16),
            pltpu.VMEM((2, LENGTH // 2, COLS), bf16),
            pltpu.VMEM((2, LENGTH // 2, COLS), bf16),
            pltpu.VMEM((2, *block), bf16),
            pltpu.VMEM((4, *block), bf16),
            pltpu.VMEM((3, *block), bf16),
            pltpu.VMEM((2, LENGTH // 2, COLS), bf16),
            pltpu.VMEM((2, LENGTH // 2, COLS), bf16),
            pltpu.VMEM((2, *block), bf16),
            pltpu.VMEM((LENGTH, GROUP * COLS), bf16),
            pltpu.VMEM((LENGTH, 512), bf16),
            dma((5,)),
            dma((1,)),
            dma((count,)),
            dma((40,)),
            dma((40,)),
        ],
        compiler_params=pltpu.CompilerParams(
            collective_id=0, has_side_effects=True, vmem_limit_bytes=48 * 1024 * 1024
        ),
    )(
        packed,
        content_expand_matrix,
        switch_expand_matrix,
        contract_matrix.T,
        incoming_features,
        jnp.stack((attend_prenormal_scale, perceptron_scale)),
        forgetting_shift[None],
        spike_forget_logarithm,
        attend_unit_scale[None],
        content_kernel,
        switch_kernel,
    )


def solution(mesh):
    placed = (
        P(("rep", "fs"), "tp"),
        P(),
        P("fs", "tp"),
        P("fs", "tp"),
        P("fs", "tp"),
        P("fs", "tp"),
        P("fs", "tp"),
        P("tp"),
        P(("rep", "fs"), "tp"),
        P("tp"),
        P("tp", "fs"),
        P(),
        P("fs", "tp"),
        P("fs", "tp"),
        P(None, "tp"),
        P(None, "tp"),
        P("tp", "fs"),
    )
    return jax.shard_map(
        shards, mesh=mesh, in_specs=placed, out_specs=P(("rep", "fs"), "tp"), check_vma=False
    )
```

```python
import functools
import heapq

import jax
import jax.numpy as jnp
from jax import lax
from jax.experimental import pallas as pl
from jax.experimental.pallas import tpu as pltpu
from jax.sharding import PartitionSpec as P

HEAD_K = 32
HEAD_V = 64
SUB = 16
NEVER = -1e30
norm_eps = 1e-06
MESH = pl.DeviceIdType.MESH
WIDTH = 2176
PARTS = (
    (0, "A", 0, 256),
    (0, "B", 256, 640),
    (1, "A", 640, 1280),
    (1, "B", 1280, 2176),
)
LENGTH = 192
GROUP = 8
COLS = 256
GELU = 0.7978845608028654

ROWS = 64
SIZES = {"y": 4, "z": 8}


def tree_messages(cls, tree, lo, hi):
    first, second = ("y", "z") if tree == "A" else ("z", "y")
    msgs = []

    def chain(axis, base, deps, stage):
        n = SIZES[axis]
        made = []
        for sign in (1, -1):
            d, s = deps, stage
            for k in range(1, n // 2 + 1):
                o = dict(base)
                o[axis] = sign * (k - 1)
                r0, rn = 0, ROWS
                if k == n // 2:
                    rn = ROWS // 2
                    r0 = 0 if sign > 0 else rn
                m = dict(
                    cls=cls, lo=lo, hi=hi, axis=axis, sign=sign, o=o, r0=r0, rn=rn, deps=d, off=sign * k, stage=s
                )
                msgs.append(m)
                made.append(m)
                d, s = (m,), s + 1
        return made

    made = chain(first, {"y": 0, "z": 0}, (), 0)
    chain(second, {"y": 0, "z": 0}, (), 0)
    far = SIZES[first] // 2
    for m in made:
        if abs(m["off"]) < far:
            chain(second, {first: m["off"], second: 0}, (m,), m["stage"] + 1)
    halves = tuple(m for m in made if abs(m["off"]) == far)
    chain(second, {first: far, second: 0}, halves, halves[0]["stage"] + 1)
    return msgs


def plan(parts, rate, lat, each):
    msgs = []
    for p in parts:
        msgs += tree_messages(*p)
    kids = {}
    for i, m in enumerate(msgs):
        m["id"] = i
        m["bytes"] = m["rn"] * (m["hi"] - m["lo"]) * 2
        m["need"] = len(m["deps"])
        for d in m["deps"]:
            kids.setdefault(d["id"], []).append(m)
    depth = {}

    def depth_of(m):
        if m["id"] not in depth:
            depth[m["id"]] = 1 + max((depth_of(k) for k in kids.get(m["id"], ())), default=0)
        return depth[m["id"]]

    groups = {}
    for m in msgs:
        m["dz"] = m["o"]["z"] + (m["sign"] if m["axis"] == "z" else 0)
        m["dz"] = 4 if abs(m["dz"]) == 4 else m["dz"]
        leaf = not kids.get(m["id"])
        key = (m["lo"], m["axis"], m["dz"]) if leaf else m["id"]
        groups.setdefault(key, []).append(m)
    for i, members in enumerate(groups.values()):
        for m in members:
            m["sem"] = i
            shared = not kids.get(m["id"])
            m["leaves"] = sum(k["rn"] for k in members) if shared else None
    free = {(a, s): 0.0 for a in "yz" for s in (1, -1)}
    avail = {k: [] for k in free}
    events = [(0.0, 0, m["id"]) for m in msgs if not m["deps"]]
    heapq.heapify(events)
    order = []
    while events:
        t = events[0][0]
        while events and events[0][0] <= t + 1e-9:
            _, kind, i = heapq.heappop(events)
            if kind == 0:
                m = msgs[i]
                heapq.heappush(avail[(m["axis"], m["sign"])], (m["cls"], -depth_of(m), i))
        for link, queue in avail.items():
            if queue and free[link] <= t + 1e-9:
                m = msgs[heapq.heappop(queue)[2]]
                m["start"] = t
                free[link] = t + m["bytes"] / rate + each
                m["arrive"] = free[link] + lat
                order.append(m)
                heapq.heappush(events, (free[link], 1, 0))
                for k in kids.get(m["id"], ()):
                    k["need"] -= 1
                    if k["need"] == 0:
                        heapq.heappush(events, (m["arrive"], 0, k["id"]))
    for members in groups.values():
        last = max(members, key=lambda m: m["arrive"])
        for m in members:
            m["final"] = m is last
    return order


def neighbour(axis, sign):
    rep, fs = lax.axis_index("rep"), lax.axis_index("fs")
    y, z = lax.rem(fs, 4), rep * 8 + fs // 4
    if axis == "y":
        y = lax.rem(y + 4 + sign, 4)
    else:
        z = lax.rem(z + 16 + sign, 16)
    return {"rep": z // 8, "fs": lax.rem(z, 8) * 4 + y}


def block_of(o):
    fs = lax.axis_index("fs")
    y, z = lax.rem(fs, 4), fs // 4
    y = lax.rem(y + 8 - o["y"], 4)
    z = lax.rem(z + 16 - o["z"], 8)
    return z * 4 + y


def attention_pieces(q, k, v, g, ld, unit, roll):
    length = q.shape[0]
    blocks = length // SUB
    exact = lax.Precision.HIGHEST
    row = lax.broadcasted_iota(jnp.int32, (length, 64), 0) % SUB
    c = ld
    shift = 1
    while shift < SUB:
        c = c + jnp.where(row >= shift, roll(c, shift), 0.0)
        shift *= 2
    key_head = lax.broadcasted_iota(jnp.int32, (64, 128), 0) // HEAD_K
    value_head = lax.broadcasted_iota(jnp.int32, (64, 128), 1) // HEAD_V
    spread = jnp.where(key_head == value_head, 1.0, 0.0)
    c3 = c.reshape(blocks, SUB, 64)
    total = c3[:, SUB - 1 : SUB, :]
    k_end = (k.reshape(blocks, SUB, 64) * jnp.exp(total - c3))
    q_in = q * jnp.exp(c)
    v3 = v.reshape(blocks, SUB, 128)
    fade = jnp.exp(total)
    q3 = q_in.reshape(blocks, SUB, 64)
    own_head = (
        lax.broadcasted_iota(jnp.int32, (128, 64), 0) // HEAD_V
        == lax.broadcasted_iota(jnp.int32, (128, 64), 1) // HEAD_K
    )
    yield None
    out = jnp.zeros((length, 128), jnp.float32)
    for j in range(SUB):
        if j == 0:
            pairs, values = q * k, v
        else:
            differ = jnp.where(row >= j, c - roll(c, j), NEVER)
            pairs, values = q * roll(k, j) * jnp.exp(differ), roll(v, j)
        scores = jnp.dot(pairs, spread, precision=exact, preferred_element_type=jnp.float32)
        out = out + scores * values
        if j % 4 == 3:
            yield None
    state = None
    carried = [jnp.zeros((SUB, 128), jnp.float32)]
    for i in range(blocks):
        if state is not None:
            carried.append(
                lax.dot_general(
                    q3[i], state, (((1,), (1,)), ((), ())), precision=exact,
                    preferred_element_type=jnp.float32,
                )
            )
        if i < blocks - 1:
            update = lax.dot_general(
                v3[i], k_end[i], (((0,), (0,)), ((), ())), precision=exact,
                preferred_element_type=jnp.float32,
            )
            update = jnp.where(own_head, update, 0.0)
            state = update if state is None else state * fade[i] + update
        if i % 4 == 3:
            yield None
    out = out + jnp.concatenate(carried, axis=0)
    same = jnp.where(
        lax.broadcasted_iota(jnp.int32, (128, 128), 0) // HEAD_V
        == lax.broadcasted_iota(jnp.int32, (128, 128), 1) // HEAD_V,
        1.0 / HEAD_V,
        0.0,
    )
    mean = jnp.dot(out * out, same, precision=exact, preferred_element_type=jnp.float32)
    out = out * lax.rsqrt(mean + norm_eps) * unit * (g / (1.0 + jnp.exp(-g)))
    yield out.astype(jnp.bfloat16)


def rows_norm(blocks, gain_ref, out):
    total = jnp.zeros((LENGTH, COLS), jnp.float32)
    for t in range(GROUP):
        one = blocks[t].astype(jnp.float32)
        total = total + one * one
    mean = jnp.sum(total, axis=1, keepdims=True) * (1.0 / (GROUP * COLS))
    scale = lax.rsqrt(mean + norm_eps)
    for t in range(GROUP):
        at = slice(t * COLS, (t + 1) * COLS)
        gain = gain_ref[at].astype(jnp.float32).reshape(1, COLS)
        out[:, at] = (blocks[t].astype(jnp.float32) * scale * gain).astype(jnp.bfloat16)


def short_conv(tokens, taps):
    row = lax.broadcasted_iota(jnp.int32, tokens.shape, 0)
    one = jnp.where(row >= 1, pltpu.roll(tokens, 1, 0), 0.0)
    two = jnp.where(row >= 2, pltpu.roll(tokens, 2, 0), 0.0)
    return two * taps[0:1] + one * taps[1:2] + tokens * taps[2:3]


def layer_kernel(
    order,
    query_ref,
    key_ref,
    content_ref,
    switch_ref,
    forget_ref,
    mix_ref,
    value_ref,
    gate_ref,
    down_ref,
    x_ref,
    pre_ref,
    post_ref,
    shift_ref,
    spike_ref,
    unit_ref,
    value_taps_ref,
    gate_taps_ref,
    out_ref,
    whole,
    x_all,
    mid_all,
    sums,
    from_partner,
    pair_sums,
    passing,
    passed,
    from_chips,
    down_from_partner,
    down_pair_sums,
    down_passing,
    down_passed,
    down_from_chips,
    down_sums,
    normed,
    hidden,
    raised,
    narrow,
    pre_gain,
    post_gain,
    shift_row,
    spike_turned,
    unit_row,
    value_taps,
    gate_taps,
    own_sem,
    send_sem,
    recv_sem,
    tp_send,
    tp_recv,
):
    f32, bf16 = jnp.float32, jnp.bfloat16
    tp = lax.axis_index("tp")
    chip, core = tp // 2, lax.rem(tp, 2)
    partner = chip * 2 + (1 - core)

    def peer(d):
        return lax.rem(chip + 4 + d, 4) * 2 + core

    barrier = pltpu.get_barrier_semaphore()
    for axis in ("y", "z"):
        for sign in (1, -1):
            pl.semaphore_signal(
                barrier, inc=1, device_id=neighbour(axis, sign), device_id_type=MESH
            )
    for other in (peer(1), peer(3), partner):
        pl.semaphore_signal(barrier, inc=1, device_id={"tp": other}, device_id_type=MESH)
    mine = pl.ds(pl.multiple_of(lax.axis_index("fs") * ROWS, ROWS), ROWS)
    pairs = (
        (query_ref, narrow.at[0]),
        (key_ref, narrow.at[1]),
        (forget_ref, narrow.at[2]),
        (content_ref, whole.at[mine, pl.ds(128, 128)]),
        (switch_ref, whole.at[mine, pl.ds(256, 128)]),
        (mix_ref, whole.at[mine, pl.ds(512, 128)]),
        (value_ref, whole.at[mine, pl.ds(640, 512)]),
        (gate_ref, whole.at[mine, pl.ds(1152, 512)]),
        (down_ref, whole.at[mine, pl.ds(1664, 512)]),
        (x_ref, x_all.at[tp]),
        (pre_ref, pre_gain),
        (post_ref, post_gain),
        (shift_ref, shift_row),
        (spike_ref, spike_turned),
        (unit_ref, unit_row),
        (value_taps_ref, value_taps),
        (gate_taps_ref, gate_taps),
    )
    own = [pltpu.make_async_copy(a, b, own_sem.at[i]) for i, (a, b) in enumerate(pairs)]
    for one in own:
        one.start()
    for one in own[:3]:
        one.wait()
    whole[mine, 0:128] = jnp.concatenate((narrow[0], narrow[1]), axis=1)
    whole[mine, 384:512] = jnp.concatenate((narrow[2], jnp.zeros_like(narrow[2])), axis=1)
    for one in own[3:]:
        one.wait()
    pl.semaphore_wait(barrier, 7)

    def copy_of(m, step):
        o = dict(m["o"])
        o[m["axis"]] = o[m["axis"]] + step * m["sign"]
        row = pl.multiple_of(block_of(o) * ROWS + m["r0"], 16)
        at = whole.at[pl.ds(row, m["rn"]), pl.ds(m["lo"], m["hi"] - m["lo"])]
        return pltpu.make_async_remote_copy(
            src_ref=at,
            dst_ref=at,
            send_sem=send_sem.at[0],
            recv_sem=recv_sem.at[m["sem"]],
            device_id=neighbour(m["axis"], m["sign"]),
            device_id_type=MESH,
        )

    seen, at_message = set(), [0]

    def arrived(m):
        if m["sem"] not in seen:
            seen.add(m["sem"])
            if m["leaves"] is None:
                copy_of(m, 1).wait_recv()
                return
            at = whole.at[pl.ds(0, m["leaves"]), pl.ds(m["lo"], m["hi"] - m["lo"])]
            pltpu.make_async_remote_copy(
                src_ref=at,
                dst_ref=at,
                send_sem=send_sem.at[0],
                recv_sem=recv_sem.at[m["sem"]],
                device_id=neighbour(m["axis"], m["sign"]),
                device_id_type=MESH,
            ).wait_recv()

    def pump(until):
        while at_message[0] < len(order) and order[at_message[0]]["start"] <= until:
            m = order[at_message[0]]
            for d in m["deps"]:
                arrived(d)
            copy_of(m, 0).start()
            at_message[0] += 1

    def class_arrived(cls):
        mine_of = sorted((m for m in order if m["cls"] == cls), key=lambda m: m["arrive"])
        for m in mine_of:
            if m["leaves"] is None or m["final"]:
                pump(m["arrive"])
                arrived(m)
        return mine_of[-1]["arrive"]

    def from_depth(cls, dz):
        came = [m for m in order if m["cls"] == cls and m["dz"] == dz]
        for m in sorted(came, key=lambda m: m["arrive"]):
            if m["leaves"] is None or m["final"]:
                pump(m["arrive"])
                arrived(m)

    def tp_copy(src, dst, number, to):
        return pltpu.make_async_remote_copy(
            src_ref=src,
            dst_ref=dst,
            send_sem=tp_send.at[number // 10],
            recv_sem=tp_recv.at[number],
            device_id={"tp": to},
            device_id_type=MESH,
        )

    def begin(copy):
        copy.start()

    right, left = peer(1), peer(3)
    low, high = pl.ds(0, LENGTH // 2), pl.ds(LENGTH // 2, LENGTH // 2)

    def move(buf, owner, rows, number, to):
        at = buf.at[owner, rows]
        return tp_copy(at, at, number, to)

    def share(buf, base):
        begin(move(buf, tp, low, base, right))
        begin(move(buf, tp, high, base + 1, left))
        begin(move(buf, tp, high, base + 2, right))
        begin(move(buf, tp, low, base + 3, left))
        begin(tp_copy(buf.at[tp], buf.at[tp], base + 6, partner))

    def share_on(buf, base):
        move(buf, left, low, base, right).wait_recv()
        begin(move(buf, left, low, base + 4, right))
        move(buf, right, high, base + 1, left).wait_recv()
        begin(move(buf, right, high, base + 5, left))
        move(buf, left, high, base + 2, right).wait_recv()
        begin(tp_copy(buf.at[left], buf.at[left], base + 7, partner))
        move(buf, right, low, base + 3, left).wait_recv()
        begin(tp_copy(buf.at[right], buf.at[right], base + 8, partner))

    def shared(buf, base):
        far = peer(2)
        move(buf, far, low, base + 4, right).wait_recv()
        move(buf, far, high, base + 5, left).wait_recv()
        begin(tp_copy(buf.at[far], buf.at[far], base + 9, partner))
        for k, d in enumerate((0, 3, 1, 2)):
            came = buf.at[lax.rem(chip + d, 4) * 2 + (1 - core)]
            tp_copy(came, came, base + 6 + k, partner).wait_recv()

    def summed(product, sums, got, paired, through, joined, chips, base, clock):
        def products(d, before):
            there = lax.rem(chip + d, 4) * 2
            sums[there + 1 - core] = product(there + 1 - core).astype(bf16)
            if before is not None:
                begin(before)
            sums[there + core] = product(there + core).astype(bf16)
            return tp_copy(sums.at[there + 1 - core], got.at[d], base + d, partner)

        def pair(d):
            there = lax.rem(chip + d, 4) * 2 + core
            tp_copy(sums.at[there], got.at[d], base + d, partner).wait_recv()
            paired[d - 1] = (sums[there].astype(f32) + got[d].astype(f32)).astype(bf16)

        ready = products(2, None)
        begin(ready)
        ready = products(1, None)
        begin(ready)
        ready = products(3, None)
        begin(ready)
        pair(2)
        ready = products(0, None)
        begin(tp_copy(paired.at[1, low], through.at[0], base + 4, right))
        begin(tp_copy(paired.at[1, high], through.at[1], base + 5, left))
        begin(ready)
        pair(1)
        pair(3)
        begin(tp_copy(paired.at[0, high], chips.at[0, high], base + 6, right))
        tp_copy(sums.at[tp], got.at[0], base, partner).wait_recv()
        total = sums[tp].astype(f32) + got[0].astype(f32)
        begin(tp_copy(paired.at[2, low], chips.at[1, low], base + 7, left))
        clock()
        tp_copy(through.at[0], through.at[0], base + 4, right).wait_recv()
        half = LENGTH // 2
        joined[0] = (paired[0, 0:half].astype(f32) + through[0].astype(f32)).astype(bf16)
        tp_copy(through.at[1], through.at[1], base + 5, left).wait_recv()
        joined[1] = (paired[2, half:].astype(f32) + through[1].astype(f32)).astype(bf16)
        begin(tp_copy(joined.at[0], chips.at[0, low], base + 8, right))
        begin(tp_copy(joined.at[1], chips.at[1, high], base + 9, left))
        clock()
        tp_copy(chips.at[0, high], chips.at[0, high], base + 6, right).wait_recv()
        tp_copy(chips.at[1, low], chips.at[1, low], base + 7, left).wait_recv()
        tp_copy(chips.at[0, low], chips.at[0, low], base + 8, right).wait_recv()
        tp_copy(chips.at[1, high], chips.at[1, high], base + 9, left).wait_recv()
        return total + chips[0].astype(f32) + chips[1].astype(f32)

    share(x_all, 0)
    pump(T_SHARE)
    share_on(x_all, 0)
    pump(T_SHARED)
    shared(x_all, 0)
    rows_norm(x_all, pre_gain, normed)
    now = class_arrived(0)

    first = jnp.dot(normed[...], whole[:, 0:256], preferred_element_type=f32)
    second = jnp.dot(normed[...], whole[:, 256:512], preferred_element_type=f32)
    pump(now + 2.0)
    rounded = first.astype(bf16).astype(f32)
    query = rounded[:, 0:64] * HEAD_K ** (-0.5)
    key = rounded[:, 64:128]
    value = rounded[:, 128:256]
    gate = second[:, 0:128].astype(bf16).astype(f32)
    forget = second[:, 128:192] + shift_row[...]
    decay = -(jnp.maximum(-forget, 0.0) + jnp.log1p(jnp.exp(-jnp.abs(forget)))) / 16.0
    decay = decay + spike_turned[...].T
    unit = unit_row[...].astype(f32)
    now = now + 2.0
    for piece in attention_pieces(
        query, key, value, gate, decay, unit, lambda a, s: pltpu.roll(a, s, 0)
    ):
        now = now + T_PIECE
        pump(now)
        gated = piece

    def mix_part(t):
        rows = pl.ds(pl.multiple_of(t * COLS, COLS), COLS)
        return lax.dot_general(
            gated, whole[rows, 512:640], (((1,), (1,)), ((), ())), preferred_element_type=f32
        )

    ticks = [now]

    def tick(step):
        ticks[0] = ticks[0] + step
        pump(ticks[0])

    total = summed(
        mix_part, sums, from_partner, pair_sums, passing, passed, from_chips, 10, lambda: tick(T_SUM)
    )
    mix = total.astype(bf16)
    mid_all[tp] = (x_all[tp].astype(f32) + mix.astype(f32)).astype(bf16)
    tick(T_MID)
    share(mid_all, 20)
    tick(T_MID)
    share_on(mid_all, 20)
    tick(T_MID)
    shared(mid_all, 20)
    rows_norm(mid_all, post_gain, normed)
    for dz in (0, 1, -1, 2, -2, 3, -3, 4):
        from_depth(1, dz)
        z = lax.rem(lax.axis_index("fs") // 4 + 16 - dz, 8)
        deep = pl.ds(pl.multiple_of(z * 256, 256), 256)
        for at in (0, 512):
            part = jnp.dot(
                normed[:, deep], whole[deep, 640 + at : 1152 + at], preferred_element_type=f32
            )
            if dz == 0:
                raised[:, at : at + 512] = part
            else:
                raised[:, at : at + 512] = raised[:, at : at + 512] + part
    class_arrived(1)
    pump(1e9)

    for block in range(4):
        at = block * 128
        cols = slice(at, at + 128)
        up_value = raised[:, at : at + 128]
        up_gate = raised[:, 512 + at : 640 + at]
        conv_value = short_conv(up_value.astype(bf16).astype(f32), value_taps[:, cols].astype(f32))
        conv_gate = short_conv(up_gate.astype(bf16).astype(f32), gate_taps[:, cols].astype(f32))
        cube = conv_gate + 0.044715 * (conv_gate * conv_gate * conv_gate)
        gelu = conv_gate * (0.5 * (1.0 + jnp.tanh(GELU * cube)))
        hidden[:, cols] = (conv_value * gelu).astype(bf16)

    def down_part(t):
        rows = pl.ds(pl.multiple_of(t * COLS, COLS), COLS)
        return lax.dot_general(
            hidden[...], whole[rows, 1664:2176], (((1,), (1,)), ((), ())), preferred_element_type=f32
        )

    total = summed(
        down_part,
        down_sums,
        down_from_partner,
        down_pair_sums,
        down_passing,
        down_passed,
        down_from_chips,
        30,
        lambda: None,
    )
    out_ref[...] = (mid_all[tp].astype(f32) + total.astype(bf16).astype(f32)).astype(bf16)

    seven = x_all.at[pl.ds(0, 7)]
    for group in range(4):
        tp_copy(seven, seven, group * 10, partner).wait_send()
    rest = whole.at[pl.ds(0, 31 * ROWS)]
    pltpu.make_async_remote_copy(
        src_ref=rest,
        dst_ref=rest,
        send_sem=send_sem.at[0],
        recv_sem=recv_sem.at[0],
        device_id=neighbour("y", 1),
        device_id_type=MESH,
    ).wait_send()


T_SHARE = 4.0
T_SHARED = 9.0
T_PIECE = 0.7
T_SUM = 2.0
T_MID = 2.5


def shards(
    incoming_features,
    attend_prenormal_scale,
    probe_matrix,
    lookup_matrix,
    content_matrix,
    forgetting_matrix,
    result_switch_matrix,
    forgetting_shift,
    spike_forget_logarithm,
    attend_unit_scale,
    attend_result_matrix,
    perceptron_scale,
    content_expand_matrix,
    switch_expand_matrix,
    content_kernel,
    switch_kernel,
    contract_matrix,
):
    order = plan(PARTS, 44e3, 2.3, 0.07)
    count = 1 + max(m["sem"] for m in order)
    block = (LENGTH, COLS)
    dma = pltpu.SemaphoreType.DMA
    vmem = pl.BlockSpec(memory_space=pltpu.VMEM)
    hbm = pl.BlockSpec(memory_space=pl.ANY)
    bf16 = jnp.bfloat16
    return pl.pallas_call(
        functools.partial(layer_kernel, order),
        out_shape=jax.ShapeDtypeStruct(block, bf16),
        in_specs=[hbm] * 17,
        out_specs=vmem,
        scratch_shapes=[
            pltpu.VMEM((32 * ROWS, WIDTH), bf16),
            pltpu.VMEM((GROUP, *block), bf16),
            pltpu.VMEM((GROUP, *block), bf16),
            pltpu.VMEM((GROUP, *block), bf16),
            pltpu.VMEM((4, *block), bf16),
            pltpu.VMEM((3, *block), bf16),
            pltpu.VMEM((2, LENGTH // 2, COLS), bf16),
            pltpu.VMEM((2, LENGTH // 2, COLS), bf16),
            pltpu.VMEM((2, *block), bf16),
            pltpu.VMEM((4, *block), bf16),
            pltpu.VMEM((3, *block), bf16),
            pltpu.VMEM((2, LENGTH // 2, COLS), bf16),
            pltpu.VMEM((2, LENGTH // 2, COLS), bf16),
            pltpu.VMEM((2, *block), bf16),
            pltpu.VMEM((GROUP, *block), bf16),
            pltpu.VMEM((LENGTH, GROUP * COLS), bf16),
            pltpu.VMEM((LENGTH, 512), bf16),
            pltpu.VMEM((LENGTH, 1024), jnp.float32),
            pltpu.VMEM((3, ROWS, 64), bf16),
            pltpu.VMEM((2048,), bf16),
            pltpu.VMEM((2048,), bf16),
            pltpu.VMEM((1, 64), jnp.float32),
            pltpu.VMEM((64, LENGTH), jnp.float32),
            pltpu.VMEM((1, 128), bf16),
            pltpu.VMEM((3, 512), bf16),
            pltpu.VMEM((3, 512), bf16),
            dma((17,)),
            dma((1,)),
            dma((count,)),
            dma((4,)),
            dma((40,)),
        ],
        compiler_params=pltpu.CompilerParams(
            collective_id=0, has_side_effects=True, vmem_limit_bytes=67043328
        ),
    )(
        probe_matrix,
        lookup_matrix,
        content_matrix,
        result_switch_matrix,
        forgetting_matrix,
        attend_result_matrix.T,
        content_expand_matrix,
        switch_expand_matrix,
        contract_matrix.T,
        incoming_features,
        attend_prenormal_scale,
        perceptron_scale,
        forgetting_shift[None],
        spike_forget_logarithm.T,
        attend_unit_scale[None],
        content_kernel,
        switch_kernel,
    )


def solution(mesh):
    placed = (
        P(("rep", "fs"), "tp"),
        P(),
        P("fs", "tp"),
        P("fs", "tp"),
        P("fs", "tp"),
        P("fs", "tp"),
        P("fs", "tp"),
        P("tp"),
        P(("rep", "fs"), "tp"),
        P("tp"),
        P("tp", "fs"),
        P(),
        P("fs", "tp"),
        P("fs", "tp"),
        P(None, "tp"),
        P(None, "tp"),
        P("tp", "fs"),
    )
    return jax.shard_map(
        shards, mesh=mesh, in_specs=placed, out_specs=P(("rep", "fs"), "tp"), check_vma=False
    )
```

```python
import functools
import heapq

import jax
import jax.numpy as jnp
from jax import lax
from jax.experimental import pallas as pl
from jax.experimental.pallas import tpu as pltpu
from jax.sharding import PartitionSpec as P

HEAD_K = 32
HEAD_V = 64
SUB = 16
NEVER = -1e30
norm_eps = 1e-06
MESH = pl.DeviceIdType.MESH
WIDTH = 2176
PARTS = (
    (0, "A", 0, 256),
    (0, "B", 256, 640),
    (1, "A", 640, 1280),
    (1, "B", 1280, 2176),
)
LENGTH = 192
GROUP = 8
COLS = 256
GELU = 0.7978845608028654

ROWS = 64
SIZES = {"y": 4, "z": 8}


def tree_messages(cls, tree, lo, hi):
    first, second = ("y", "z") if tree == "A" else ("z", "y")
    msgs = []

    def chain(axis, base, deps, stage):
        n = SIZES[axis]
        made = []
        for sign in (1, -1):
            d, s = deps, stage
            for k in range(1, n // 2 + 1):
                o = dict(base)
                o[axis] = sign * (k - 1)
                r0, rn = 0, ROWS
                if k == n // 2:
                    rn = ROWS // 2
                    r0 = 0 if sign > 0 else rn
                m = dict(
                    cls=cls, lo=lo, hi=hi, axis=axis, sign=sign, o=o, r0=r0, rn=rn, deps=d, off=sign * k, stage=s
                )
                msgs.append(m)
                made.append(m)
                d, s = (m,), s + 1
        return made

    made = chain(first, {"y": 0, "z": 0}, (), 0)
    chain(second, {"y": 0, "z": 0}, (), 0)
    far = SIZES[first] // 2
    for m in made:
        if abs(m["off"]) < far:
            chain(second, {first: m["off"], second: 0}, (m,), m["stage"] + 1)
    halves = tuple(m for m in made if abs(m["off"]) == far)
    chain(second, {first: far, second: 0}, halves, halves[0]["stage"] + 1)
    return msgs


def plan(parts, rate, lat, each):
    msgs = []
    for p in parts:
        msgs += tree_messages(*p)
    kids = {}
    parents = {id(d) for m in msgs for d in m["deps"]}
    twins = {}
    for m in msgs:
        m["dz"] = m["o"]["z"] + (m["sign"] if m["axis"] == "z" else 0)
        m["dz"] = 4 if abs(m["dz"]) == 4 else m["dz"]
        across = m["o"]["y" if m["axis"] == "z" else "z"]
        if id(m) in parents:
            m["key"] = (m["lo"], m["axis"], across, abs(m["off"]))
        else:
            m["key"] = (m["lo"], m["axis"], m["dz"], "leaf")
        twins.setdefault(m["key"], []).append(m)
    for m in msgs:
        keys = dict.fromkeys(d["key"] for d in m["deps"])
        m["deps"] = tuple(t for k in keys for t in twins[k])
    for i, m in enumerate(msgs):
        m["id"] = i
    for m in msgs:
        m["bytes"] = m["rn"] * (m["hi"] - m["lo"]) * 2
        m["need"] = len(m["deps"])
        for d in m["deps"]:
            kids.setdefault(d["id"], []).append(m)
    depth = {}

    def depth_of(m):
        if m["id"] not in depth:
            depth[m["id"]] = 1 + max((depth_of(k) for k in kids.get(m["id"], ())), default=0)
        return depth[m["id"]]

    for i, members in enumerate(twins.values()):
        for m in members:
            m["sem"] = i
            m["together"] = sum(k["rn"] for k in members)
    free = {(a, s): 0.0 for a in "yz" for s in (1, -1)}
    avail = {k: [] for k in free}
    events = [(0.0, 0, m["id"]) for m in msgs if not m["deps"]]
    heapq.heapify(events)
    order = []
    while events:
        t = events[0][0]
        while events and events[0][0] <= t + 1e-9:
            _, kind, i = heapq.heappop(events)
            if kind == 0:
                m = msgs[i]
                heapq.heappush(avail[(m["axis"], m["sign"])], (m["cls"], -depth_of(m), i))
        for link, queue in avail.items():
            if queue and free[link] <= t + 1e-9:
                m = msgs[heapq.heappop(queue)[2]]
                m["start"] = t
                free[link] = t + m["bytes"] / rate + each
                m["arrive"] = free[link] + lat
                order.append(m)
                heapq.heappush(events, (free[link], 1, 0))
                for k in kids.get(m["id"], ()):
                    k["need"] -= 1
                    if k["need"] == 0:
                        heapq.heappush(events, (m["arrive"], 0, k["id"]))
    for members in twins.values():
        last = max(members, key=lambda m: m["arrive"])
        for m in members:
            m["final"] = m is last
    return order


def neighbour(axis, sign):
    rep, fs = lax.axis_index("rep"), lax.axis_index("fs")
    y, z = lax.rem(fs, 4), rep * 8 + fs // 4
    if axis == "y":
        y = lax.rem(y + 4 + sign, 4)
    else:
        z = lax.rem(z + 16 + sign, 16)
    return {"rep": z // 8, "fs": lax.rem(z, 8) * 4 + y}


def block_of(o):
    fs = lax.axis_index("fs")
    y, z = lax.rem(fs, 4), fs // 4
    y = lax.rem(y + 8 - o["y"], 4)
    z = lax.rem(z + 16 - o["z"], 8)
    return z * 4 + y


def attention_pieces(q, k, v, g, ld, unit, roll):
    length = q.shape[0]
    blocks = length // SUB
    exact = lax.Precision.HIGHEST
    row = lax.broadcasted_iota(jnp.int32, (length, 64), 0) % SUB
    c = ld
    shift = 1
    while shift < SUB:
        c = c + jnp.where(row >= shift, roll(c, shift), 0.0)
        shift *= 2
    key_head = lax.broadcasted_iota(jnp.int32, (64, 128), 0) // HEAD_K
    value_head = lax.broadcasted_iota(jnp.int32, (64, 128), 1) // HEAD_V
    spread = jnp.where(key_head == value_head, 1.0, 0.0)
    c3 = c.reshape(blocks, SUB, 64)
    total = c3[:, SUB - 1 : SUB, :]
    k_end = (k.reshape(blocks, SUB, 64) * jnp.exp(total - c3))
    q_in = q * jnp.exp(c)
    v3 = v.reshape(blocks, SUB, 128)
    fade = jnp.exp(total)
    q3 = q_in.reshape(blocks, SUB, 64)
    own_head = (
        lax.broadcasted_iota(jnp.int32, (128, 64), 0) // HEAD_V
        == lax.broadcasted_iota(jnp.int32, (128, 64), 1) // HEAD_K
    )
    yield None
    out = jnp.zeros((length, 128), jnp.float32)
    for j in range(SUB):
        if j == 0:
            pairs, values = q * k, v
        else:
            differ = jnp.where(row >= j, c - roll(c, j), NEVER)
            pairs, values = q * roll(k, j) * jnp.exp(differ), roll(v, j)
        scores = jnp.dot(pairs, spread, precision=exact, preferred_element_type=jnp.float32)
        out = out + scores * values
        if j % 4 == 3:
            yield None
    state = None
    carried = [jnp.zeros((SUB, 128), jnp.float32)]
    for i in range(blocks):
        if state is not None:
            carried.append(
                lax.dot_general(
                    q3[i], state, (((1,), (1,)), ((), ())), precision=exact,
                    preferred_element_type=jnp.float32,
                )
            )
        if i < blocks - 1:
            update = lax.dot_general(
                v3[i], k_end[i], (((0,), (0,)), ((), ())), precision=exact,
                preferred_element_type=jnp.float32,
            )
            update = jnp.where(own_head, update, 0.0)
            state = update if state is None else state * fade[i] + update
        if i % 4 == 3:
            yield None
    out = out + jnp.concatenate(carried, axis=0)
    same = jnp.where(
        lax.broadcasted_iota(jnp.int32, (128, 128), 0) // HEAD_V
        == lax.broadcasted_iota(jnp.int32, (128, 128), 1) // HEAD_V,
        1.0 / HEAD_V,
        0.0,
    )
    mean = jnp.dot(out * out, same, precision=exact, preferred_element_type=jnp.float32)
    out = out * lax.rsqrt(mean + norm_eps) * unit * (g / (1.0 + jnp.exp(-g)))
    yield out.astype(jnp.bfloat16)


def rows_norm(blocks, gain_ref, out):
    total = jnp.zeros((LENGTH, COLS), jnp.float32)
    for t in range(GROUP):
        one = blocks[t].astype(jnp.float32)
        total = total + one * one
    mean = jnp.sum(total, axis=1, keepdims=True) * (1.0 / (GROUP * COLS))
    scale = lax.rsqrt(mean + norm_eps)
    for t in range(GROUP):
        at = slice(t * COLS, (t + 1) * COLS)
        gain = gain_ref[at].astype(jnp.float32).reshape(1, COLS)
        out[:, at] = (blocks[t].astype(jnp.float32) * scale * gain).astype(jnp.bfloat16)


def short_conv(tokens, taps):
    row = lax.broadcasted_iota(jnp.int32, tokens.shape, 0)
    one = jnp.where(row >= 1, pltpu.roll(tokens, 1, 0), 0.0)
    two = jnp.where(row >= 2, pltpu.roll(tokens, 2, 0), 0.0)
    return two * taps[0:1] + one * taps[1:2] + tokens * taps[2:3]


def layer_kernel(
    order,
    query_ref,
    key_ref,
    content_ref,
    switch_ref,
    forget_ref,
    mix_ref,
    value_ref,
    gate_ref,
    down_ref,
    x_ref,
    pre_ref,
    post_ref,
    shift_ref,
    spike_ref,
    unit_ref,
    value_taps_ref,
    gate_taps_ref,
    out_ref,
    whole,
    x_all,
    mid_all,
    sums,
    from_partner,
    pair_sums,
    passing,
    passed,
    from_chips,
    down_from_partner,
    down_pair_sums,
    down_passing,
    down_passed,
    down_from_chips,
    down_sums,
    normed,
    hidden,
    raised,
    narrow,
    pre_gain,
    post_gain,
    shift_row,
    spike_turned,
    unit_row,
    value_taps,
    gate_taps,
    own_sem,
    send_sem,
    recv_sem,
    tp_send,
    tp_recv,
):
    f32, bf16 = jnp.float32, jnp.bfloat16
    tp = lax.axis_index("tp")
    chip, core = tp // 2, lax.rem(tp, 2)
    partner = chip * 2 + (1 - core)

    def peer(d):
        return lax.rem(chip + 4 + d, 4) * 2 + core

    barrier = pltpu.get_barrier_semaphore()
    for axis in ("y", "z"):
        for sign in (1, -1):
            pl.semaphore_signal(
                barrier, inc=1, device_id=neighbour(axis, sign), device_id_type=MESH
            )
    for other in (peer(1), peer(3), partner):
        pl.semaphore_signal(barrier, inc=1, device_id={"tp": other}, device_id_type=MESH)
    mine = pl.ds(pl.multiple_of(lax.axis_index("fs") * ROWS, ROWS), ROWS)
    pairs = (
        (query_ref, narrow.at[0], 0),
        (key_ref, narrow.at[1], 0),
        (forget_ref, narrow.at[2], 0),
        (content_ref, whole.at[mine, pl.ds(128, 128)], 1),
        (switch_ref, whole.at[mine, pl.ds(256, 128)], 1),
        (mix_ref, whole.at[mine, pl.ds(512, 128)], 2),
        (value_ref, whole.at[mine, pl.ds(640, 512)], 3),
        (gate_ref, whole.at[mine, pl.ds(1152, 512)], 3),
        (down_ref, whole.at[mine, pl.ds(1664, 512)], 3),
        (x_ref, x_all.at[tp], 4),
        (pre_ref, pre_gain, 5),
        (post_ref, post_gain, 6),
        (shift_ref, shift_row, 7),
        (spike_ref, spike_turned, 8),
        (unit_ref, unit_row, 9),
        (value_taps_ref, value_taps, 10),
        (gate_taps_ref, gate_taps, 11),
    )
    own = [pltpu.make_async_copy(a, b, own_sem.at[i]) for a, b, i in pairs]
    for one in own:
        one.start()

    def landed(at, number):
        pltpu.make_async_copy(at, at, own_sem.at[number]).wait()

    landed(narrow, 0)
    whole[mine, 0:128] = jnp.concatenate((narrow[0], narrow[1]), axis=1)
    whole[mine, 384:512] = jnp.concatenate((narrow[2], jnp.zeros_like(narrow[2])), axis=1)
    landed(whole.at[mine, pl.ds(128, 256)], 1)
    landed(whole.at[mine, pl.ds(640, 1536)], 3)
    for one in [own[5], *own[9:]]:
        one.wait()
    pl.semaphore_wait(barrier, 7)

    def copy_of(m, step):
        o = dict(m["o"])
        o[m["axis"]] = o[m["axis"]] + step * m["sign"]
        row = pl.multiple_of(block_of(o) * ROWS + m["r0"], 16)
        at = whole.at[pl.ds(row, m["rn"]), pl.ds(m["lo"], m["hi"] - m["lo"])]
        return pltpu.make_async_remote_copy(
            src_ref=at,
            dst_ref=at,
            send_sem=send_sem.at[0],
            recv_sem=recv_sem.at[m["sem"]],
            device_id=neighbour(m["axis"], m["sign"]),
            device_id_type=MESH,
        )

    seen, at_message = set(), [0]

    def arrived(m):
        if m["sem"] not in seen:
            seen.add(m["sem"])
            at = whole.at[pl.ds(0, m["together"]), pl.ds(m["lo"], m["hi"] - m["lo"])]
            pltpu.make_async_remote_copy(
                src_ref=at,
                dst_ref=at,
                send_sem=send_sem.at[0],
                recv_sem=recv_sem.at[m["sem"]],
                device_id=neighbour(m["axis"], m["sign"]),
                device_id_type=MESH,
            ).wait_recv()

    def pump(until):
        while at_message[0] < len(order) and order[at_message[0]]["start"] <= until:
            m = order[at_message[0]]
            for d in m["deps"]:
                arrived(d)
            copy_of(m, 0).start()
            at_message[0] += 1

    def class_arrived(cls):
        mine_of = sorted((m for m in order if m["cls"] == cls), key=lambda m: m["arrive"])
        for m in mine_of:
            if m["final"]:
                pump(m["arrive"])
                arrived(m)
        return mine_of[-1]["arrive"]

    def from_depth(cls, dz):
        came = [m for m in order if m["cls"] == cls and m["dz"] == dz]
        for m in sorted(came, key=lambda m: m["arrive"]):
            if m["final"]:
                pump(m["arrive"])
                arrived(m)

    def tp_copy(src, dst, number, to):
        return pltpu.make_async_remote_copy(
            src_ref=src,
            dst_ref=dst,
            send_sem=tp_send.at[number // 10],
            recv_sem=tp_recv.at[number],
            device_id={"tp": to},
            device_id_type=MESH,
        )

    def begin(copy):
        copy.start()

    right, left = peer(1), peer(3)
    low, high = pl.ds(0, LENGTH // 2), pl.ds(LENGTH // 2, LENGTH // 2)

    def move(buf, owner, rows, number, to):
        at = buf.at[owner, rows]
        return tp_copy(at, at, number, to)

    def share(buf, base, clock):
        begin(move(buf, tp, low, base, right))
        begin(move(buf, tp, high, base + 1, left))
        begin(move(buf, tp, high, base + 2, right))
        begin(move(buf, tp, low, base + 3, left))
        begin(tp_copy(buf.at[tp], buf.at[tp], base + 6, partner))
        clock(1.5)
        clock(1.5)
        move(buf, left, low, base, right).wait_recv()
        begin(move(buf, left, low, base + 4, right))
        move(buf, right, high, base + 1, left).wait_recv()
        begin(move(buf, right, high, base + 5, left))
        clock(1.0)
        move(buf, left, high, base + 2, right).wait_recv()
        begin(tp_copy(buf.at[left], buf.at[left], base + 7, partner))
        move(buf, right, low, base + 3, left).wait_recv()
        begin(tp_copy(buf.at[right], buf.at[right], base + 8, partner))
        clock(1.0)
        clock(1.0)
        far = peer(2)
        move(buf, far, low, base + 4, right).wait_recv()
        move(buf, far, high, base + 5, left).wait_recv()
        begin(tp_copy(buf.at[far], buf.at[far], base + 9, partner))
        clock(1.0)
        for k, d in enumerate((0, 3, 1, 2)):
            came = buf.at[lax.rem(chip + d, 4) * 2 + (1 - core)]
            tp_copy(came, came, base + 6 + k, partner).wait_recv()

    def summed(product, sums, got, paired, through, joined, chips, base, clock):
        def products(d):
            there = lax.rem(chip + d, 4) * 2
            sums[there + 1 - core] = product(there + 1 - core).astype(bf16)
            sums[there + core] = product(there + core).astype(bf16)
            return tp_copy(sums.at[there + 1 - core], got.at[d], base + d, partner)

        def pair(d):
            there = lax.rem(chip + d, 4) * 2 + core
            tp_copy(sums.at[there], got.at[d], base + d, partner).wait_recv()
            paired[d - 1] = (sums[there].astype(f32) + got[d].astype(f32)).astype(bf16)

        for d in (2, 1, 3):
            begin(products(d))
            clock(0.25)
        clock(0.5)
        pair(2)
        ready = products(0)
        begin(tp_copy(paired.at[1, low], through.at[0], base + 4, right))
        begin(tp_copy(paired.at[1, high], through.at[1], base + 5, left))
        begin(ready)
        clock(0.5)
        pair(1)
        pair(3)
        begin(tp_copy(paired.at[0, high], chips.at[0, high], base + 6, right))
        tp_copy(sums.at[tp], got.at[0], base, partner).wait_recv()
        total = sums[tp].astype(f32) + got[0].astype(f32)
        begin(tp_copy(paired.at[2, low], chips.at[1, low], base + 7, left))
        clock(1.2)
        clock(1.2)
        tp_copy(through.at[0], through.at[0], base + 4, right).wait_recv()
        half = LENGTH // 2
        joined[0] = (paired[0, 0:half].astype(f32) + through[0].astype(f32)).astype(bf16)
        tp_copy(through.at[1], through.at[1], base + 5, left).wait_recv()
        joined[1] = (paired[2, half:].astype(f32) + through[1].astype(f32)).astype(bf16)
        begin(tp_copy(joined.at[0], chips.at[0, low], base + 8, right))
        begin(tp_copy(joined.at[1], chips.at[1, high], base + 9, left))
        clock(1.3)
        clock(1.3)
        tp_copy(chips.at[0, high], chips.at[0, high], base + 6, right).wait_recv()
        tp_copy(chips.at[1, low], chips.at[1, low], base + 7, left).wait_recv()
        tp_copy(chips.at[0, low], chips.at[0, low], base + 8, right).wait_recv()
        tp_copy(chips.at[1, high], chips.at[1, high], base + 9, left).wait_recv()
        return total + chips[0].astype(f32) + chips[1].astype(f32)

    ticks = [0.5]

    def tick(step):
        ticks[0] = ticks[0] + step
        pump(ticks[0])

    def still(step):
        del step

    share(x_all, 0, tick)
    rows_norm(x_all, pre_gain, normed)
    ticks[0] = class_arrived(0)

    first = jnp.dot(normed[...], whole[:, 0:256], preferred_element_type=f32)
    second = jnp.dot(normed[...], whole[:, 256:512], preferred_element_type=f32)
    tick(0.7)
    rounded = first.astype(bf16).astype(f32)
    query = rounded[:, 0:64] * HEAD_K ** (-0.5)
    key = rounded[:, 64:128]
    value = rounded[:, 128:256]
    gate = second[:, 0:128].astype(bf16).astype(f32)
    forget = second[:, 128:192] + shift_row[...]
    decay = -(jnp.maximum(-forget, 0.0) + jnp.log1p(jnp.exp(-jnp.abs(forget)))) / 16.0
    decay = decay + spike_turned[...].T
    unit = unit_row[...].astype(f32)
    for piece in attention_pieces(
        query, key, value, gate, decay, unit, lambda a, s: pltpu.roll(a, s, 0)
    ):
        tick(T_PIECE)
        gated = piece

    def mix_part(t):
        rows = pl.ds(pl.multiple_of(t * COLS, COLS), COLS)
        return lax.dot_general(
            gated, whole[rows, 512:640], (((1,), (1,)), ((), ())), preferred_element_type=f32
        )

    total = summed(
        mix_part, sums, from_partner, pair_sums, passing, passed, from_chips, 10, tick
    )
    mix = total.astype(bf16)
    mid_all[tp] = (x_all[tp].astype(f32) + mix.astype(f32)).astype(bf16)
    share(mid_all, 20, tick)
    rows_norm(mid_all, post_gain, normed)
    last_of = {}
    for m in order:
        if m["cls"] == 1:
            last_of[m["dz"]] = max(last_of.get(m["dz"], 0.0), m["arrive"])
    by_arrival = sorted(last_of, key=last_of.get)
    for dz in by_arrival:
        from_depth(1, dz)
        z = lax.rem(lax.axis_index("fs") // 4 + 16 - dz, 8)
        deep = pl.ds(pl.multiple_of(z * 256, 256), 256)
        for at in (0, 512):
            part = jnp.dot(
                normed[:, deep], whole[deep, 640 + at : 1152 + at], preferred_element_type=f32
            )
            if dz == by_arrival[0]:
                raised[:, at : at + 512] = part
            else:
                raised[:, at : at + 512] = raised[:, at : at + 512] + part
    class_arrived(1)
    pump(1e9)

    for block in range(4):
        at = block * 128
        cols = slice(at, at + 128)
        up_value = raised[:, at : at + 128]
        up_gate = raised[:, 512 + at : 640 + at]
        conv_value = short_conv(up_value.astype(bf16).astype(f32), value_taps[:, cols].astype(f32))
        conv_gate = short_conv(up_gate.astype(bf16).astype(f32), gate_taps[:, cols].astype(f32))
        cube = conv_gate + 0.044715 * (conv_gate * conv_gate * conv_gate)
        gelu = conv_gate * (0.5 * (1.0 + jnp.tanh(GELU * cube)))
        hidden[:, cols] = (conv_value * gelu).astype(bf16)

    def down_part(t):
        rows = pl.ds(pl.multiple_of(t * COLS, COLS), COLS)
        return lax.dot_general(
            hidden[...], whole[rows, 1664:2176], (((1,), (1,)), ((), ())), preferred_element_type=f32
        )

    total = summed(
        down_part,
        down_sums,
        down_from_partner,
        down_pair_sums,
        down_passing,
        down_passed,
        down_from_chips,
        30,
        still,
    )
    out_ref[...] = (mid_all[tp].astype(f32) + total.astype(bf16).astype(f32)).astype(bf16)

    seven = x_all.at[pl.ds(0, 7)]
    for group in range(4):
        tp_copy(seven, seven, group * 10, partner).wait_send()
    rest = whole.at[pl.ds(0, 31 * ROWS)]
    pltpu.make_async_remote_copy(
        src_ref=rest,
        dst_ref=rest,
        send_sem=send_sem.at[0],
        recv_sem=recv_sem.at[0],
        device_id=neighbour("y", 1),
        device_id_type=MESH,
    ).wait_send()


T_PIECE = 0.55


def shards(
    incoming_features,
    attend_prenormal_scale,
    probe_matrix,
    lookup_matrix,
    content_matrix,
    forgetting_matrix,
    result_switch_matrix,
    forgetting_shift,
    spike_forget_logarithm,
    attend_unit_scale,
    attend_result_matrix,
    perceptron_scale,
    content_expand_matrix,
    switch_expand_matrix,
    content_kernel,
    switch_kernel,
    contract_matrix,
):
    order = plan(PARTS, 46.6e3, 1.8, 0.02)
    count = 1 + max(m["sem"] for m in order)
    block = (LENGTH, COLS)
    dma = pltpu.SemaphoreType.DMA
    vmem = pl.BlockSpec(memory_space=pltpu.VMEM)
    hbm = pl.BlockSpec(memory_space=pltpu.HBM)
    bf16 = jnp.bfloat16
    return pl.pallas_call(
        functools.partial(layer_kernel, order),
        out_shape=jax.ShapeDtypeStruct(block, bf16),
        in_specs=[hbm] * 17,
        out_specs=vmem,
        scratch_shapes=[
            pltpu.VMEM((32 * ROWS, WIDTH), bf16),
            pltpu.VMEM((GROUP, *block), bf16),
            pltpu.VMEM((GROUP, *block), bf16),
            pltpu.VMEM((GROUP, *block), bf16),
            pltpu.VMEM((4, *block), bf16),
            pltpu.VMEM((3, *block), bf16),
            pltpu.VMEM((2, LENGTH // 2, COLS), bf16),
            pltpu.VMEM((2, LENGTH // 2, COLS), bf16),
            pltpu.VMEM((2, *block), bf16),
            pltpu.VMEM((4, *block), bf16),
            pltpu.VMEM((3, *block), bf16),
            pltpu.VMEM((2, LENGTH // 2, COLS), bf16),
            pltpu.VMEM((2, LENGTH // 2, COLS), bf16),
            pltpu.VMEM((2, *block), bf16),
            pltpu.VMEM((GROUP, *block), bf16),
            pltpu.VMEM((LENGTH, GROUP * COLS), bf16),
            pltpu.VMEM((LENGTH, 512), bf16),
            pltpu.VMEM((LENGTH, 1024), jnp.float32),
            pltpu.VMEM((3, ROWS, 64), bf16),
            pltpu.VMEM((2048,), bf16),
            pltpu.VMEM((2048,), bf16),
            pltpu.VMEM((1, 64), jnp.float32),
            pltpu.VMEM((64, LENGTH), jnp.float32),
            pltpu.VMEM((1, 128), bf16),
            pltpu.VMEM((3, 512), bf16),
            pltpu.VMEM((3, 512), bf16),
            dma((12,)),
            dma((1,)),
            dma((count,)),
            dma((4,)),
            dma((40,)),
        ],
        compiler_params=pltpu.CompilerParams(
            collective_id=0, has_side_effects=True, vmem_limit_bytes=67043328
        ),
    )(
        probe_matrix,
        lookup_matrix,
        content_matrix,
        result_switch_matrix,
        forgetting_matrix,
        attend_result_matrix.T,
        content_expand_matrix,
        switch_expand_matrix,
        contract_matrix.T,
        incoming_features,
        attend_prenormal_scale,
        perceptron_scale,
        forgetting_shift[None],
        spike_forget_logarithm.T,
        attend_unit_scale[None],
        content_kernel,
        switch_kernel,
    )


def solution(mesh):
    placed = (
        P(("rep", "fs"), "tp"),
        P(),
        P("fs", "tp"),
        P("fs", "tp"),
        P("fs", "tp"),
        P("fs", "tp"),
        P("fs", "tp"),
        P("tp"),
        P(("rep", "fs"), "tp"),
        P("tp"),
        P("tp", "fs"),
        P(),
        P("fs", "tp"),
        P("fs", "tp"),
        P(None, "tp"),
        P(None, "tp"),
        P("tp", "fs"),
    )
    return jax.shard_map(
        shards, mesh=mesh, in_specs=placed, out_specs=P(("rep", "fs"), "tp"), check_vma=False
    )
```

```python
import functools
import heapq

import jax
import jax.numpy as jnp
from jax import lax
from jax.experimental import pallas as pl
from jax.experimental.pallas import tpu as pltpu
from jax.sharding import PartitionSpec as P

HEAD_K = 32
HEAD_V = 64
SUB = 16
NEVER = -1e30
norm_eps = 1e-06
MESH = pl.DeviceIdType.MESH
WIDTH = 2176
PARTS = (
    (0, "A", 0, 256),
    (0, "B", 256, 640),
    (1, "A", 640, 1280),
    (1, "B", 1280, 2176),
)
LENGTH = 192
GROUP = 8
COLS = 256
GELU = 0.7978845608028654

ROWS = 64
SIZES = {"y": 4, "z": 8}


def tree_messages(cls, tree, lo, hi):
    first, second = ("y", "z") if tree == "A" else ("z", "y")
    msgs = []

    def chain(axis, base, deps, stage):
        n = SIZES[axis]
        made = []
        for sign in (1, -1):
            d, s = deps, stage
            for k in range(1, n // 2 + 1):
                o = dict(base)
                o[axis] = sign * (k - 1)
                r0, rn = 0, ROWS
                if k == n // 2:
                    rn = ROWS // 2
                    r0 = 0 if sign > 0 else rn
                m = dict(
                    cls=cls, lo=lo, hi=hi, axis=axis, sign=sign, o=o, r0=r0, rn=rn, deps=d, off=sign * k, stage=s
                )
                msgs.append(m)
                made.append(m)
                d, s = (m,), s + 1
        return made

    made = chain(first, {"y": 0, "z": 0}, (), 0)
    chain(second, {"y": 0, "z": 0}, (), 0)
    far = SIZES[first] // 2
    for m in made:
        if abs(m["off"]) < far:
            chain(second, {first: m["off"], second: 0}, (m,), m["stage"] + 1)
    halves = tuple(m for m in made if abs(m["off"]) == far)
    chain(second, {first: far, second: 0}, halves, halves[0]["stage"] + 1)
    return msgs


def plan(parts, rate, lat, each):
    msgs = []
    for p in parts:
        msgs += tree_messages(*p)
    kids = {}
    parents = {id(d) for m in msgs for d in m["deps"]}
    twins = {}
    for m in msgs:
        m["dz"] = m["o"]["z"] + (m["sign"] if m["axis"] == "z" else 0)
        m["dz"] = 4 if abs(m["dz"]) == 4 else m["dz"]
        across = m["o"]["y" if m["axis"] == "z" else "z"]
        if id(m) in parents:
            m["key"] = (m["lo"], m["axis"], across, abs(m["off"]))
        else:
            m["key"] = (m["lo"], m["axis"], m["dz"], "leaf")
        twins.setdefault(m["key"], []).append(m)
    for m in msgs:
        keys = dict.fromkeys(d["key"] for d in m["deps"])
        m["deps"] = tuple(t for k in keys for t in twins[k])
    for i, m in enumerate(msgs):
        m["id"] = i
    for m in msgs:
        m["bytes"] = m["rn"] * (m["hi"] - m["lo"]) * 2
        m["need"] = len(m["deps"])
        for d in m["deps"]:
            kids.setdefault(d["id"], []).append(m)
    depth = {}

    def depth_of(m):
        if m["id"] not in depth:
            depth[m["id"]] = 1 + max((depth_of(k) for k in kids.get(m["id"], ())), default=0)
        return depth[m["id"]]

    for i, members in enumerate(twins.values()):
        for m in members:
            m["sem"] = i
            m["together"] = sum(k["rn"] for k in members)
    free = {(a, s): 0.0 for a in "yz" for s in (1, -1)}
    avail = {k: [] for k in free}
    events = [(0.0, 0, m["id"]) for m in msgs if not m["deps"]]
    heapq.heapify(events)
    order = []
    while events:
        t = events[0][0]
        while events and events[0][0] <= t + 1e-9:
            _, kind, i = heapq.heappop(events)
            if kind == 0:
                m = msgs[i]
                m["ready"] = t
                heapq.heappush(avail[(m["axis"], m["sign"])], (m["cls"], -depth_of(m), i))
        for link, queue in avail.items():
            if queue and free[link] <= t + 1e-9:
                m = msgs[heapq.heappop(queue)[2]]
                m["start"] = t
                free[link] = t + m["bytes"] / rate + each
                m["arrive"] = free[link] + lat
                order.append(m)
                heapq.heappush(events, (free[link], 1, 0))
                for k in kids.get(m["id"], ()):
                    k["need"] -= 1
                    if k["need"] == 0:
                        heapq.heappush(events, (m["arrive"], 0, k["id"]))
    for members in twins.values():
        last = max(members, key=lambda m: m["arrive"])
        for m in members:
            m["final"] = m is last
    return order


def neighbour(axis, sign):
    rep, fs = lax.axis_index("rep"), lax.axis_index("fs")
    y, z = lax.rem(fs, 4), rep * 8 + fs // 4
    if axis == "y":
        y = lax.rem(y + 4 + sign, 4)
    else:
        z = lax.rem(z + 16 + sign, 16)
    return {"rep": z // 8, "fs": lax.rem(z, 8) * 4 + y}


def block_of(o):
    fs = lax.axis_index("fs")
    y, z = lax.rem(fs, 4), fs // 4
    y = lax.rem(y + 8 - o["y"], 4)
    z = lax.rem(z + 16 - o["z"], 8)
    return z * 4 + y


def attention_pieces(q, k, v, g, ld, unit, roll):
    length = q.shape[0]
    blocks = length // SUB
    exact = lax.Precision.HIGHEST
    row = lax.broadcasted_iota(jnp.int32, (length, 64), 0) % SUB
    c = ld
    shift = 1
    while shift < SUB:
        c = c + jnp.where(row >= shift, roll(c, shift), 0.0)
        shift *= 2
    key_head = lax.broadcasted_iota(jnp.int32, (64, 128), 0) // HEAD_K
    value_head = lax.broadcasted_iota(jnp.int32, (64, 128), 1) // HEAD_V
    spread = jnp.where(key_head == value_head, 1.0, 0.0)
    c3 = c.reshape(blocks, SUB, 64)
    total = c3[:, SUB - 1 : SUB, :]
    k_end = (k.reshape(blocks, SUB, 64) * jnp.exp(total - c3))
    q_in = q * jnp.exp(c)
    v3 = v.reshape(blocks, SUB, 128)
    fade = jnp.exp(total)
    q3 = q_in.reshape(blocks, SUB, 64)
    own_head = (
        lax.broadcasted_iota(jnp.int32, (128, 64), 0) // HEAD_V
        == lax.broadcasted_iota(jnp.int32, (128, 64), 1) // HEAD_K
    )
    yield None
    out = jnp.zeros((length, 128), jnp.float32)
    for j in range(SUB):
        if j == 0:
            pairs, values = q * k, v
        else:
            differ = jnp.where(row >= j, c - roll(c, j), NEVER)
            pairs, values = q * roll(k, j) * jnp.exp(differ), roll(v, j)
        scores = jnp.dot(pairs, spread, precision=exact, preferred_element_type=jnp.float32)
        out = out + scores * values
        if j % 4 == 3:
            yield None
    state = None
    carried = [jnp.zeros((SUB, 128), jnp.float32)]
    for i in range(blocks):
        if state is not None:
            carried.append(
                lax.dot_general(
                    q3[i], state, (((1,), (1,)), ((), ())), precision=exact,
                    preferred_element_type=jnp.float32,
                )
            )
        if i < blocks - 1:
            update = lax.dot_general(
                v3[i], k_end[i], (((0,), (0,)), ((), ())), precision=exact,
                preferred_element_type=jnp.float32,
            )
            update = jnp.where(own_head, update, 0.0)
            state = update if state is None else state * fade[i] + update
        if i % 4 == 3:
            yield None
    out = out + jnp.concatenate(carried, axis=0)
    same = jnp.where(
        lax.broadcasted_iota(jnp.int32, (128, 128), 0) // HEAD_V
        == lax.broadcasted_iota(jnp.int32, (128, 128), 1) // HEAD_V,
        1.0 / HEAD_V,
        0.0,
    )
    mean = jnp.dot(out * out, same, precision=exact, preferred_element_type=jnp.float32)
    out = out * lax.rsqrt(mean + norm_eps) * unit * (g / (1.0 + jnp.exp(-g)))
    yield out.astype(jnp.bfloat16)


def rows_norm(blocks, gain_ref, out):
    total = jnp.zeros((LENGTH, COLS), jnp.float32)
    for t in range(GROUP):
        one = blocks[t].astype(jnp.float32)
        total = total + one * one
    mean = jnp.sum(total, axis=1, keepdims=True) * (1.0 / (GROUP * COLS))
    scale = lax.rsqrt(mean + norm_eps)
    for t in range(GROUP):
        at = slice(t * COLS, (t + 1) * COLS)
        gain = gain_ref[at].astype(jnp.float32).reshape(1, COLS)
        out[:, at] = (blocks[t].astype(jnp.float32) * scale * gain).astype(jnp.bfloat16)


def short_conv(tokens, taps):
    row = lax.broadcasted_iota(jnp.int32, tokens.shape, 0)
    one = jnp.where(row >= 1, pltpu.roll(tokens, 1, 0), 0.0)
    two = jnp.where(row >= 2, pltpu.roll(tokens, 2, 0), 0.0)
    return two * taps[0:1] + one * taps[1:2] + tokens * taps[2:3]


def layer_kernel(
    order,
    query_ref,
    key_ref,
    content_ref,
    switch_ref,
    forget_ref,
    mix_ref,
    value_ref,
    gate_ref,
    down_ref,
    x_ref,
    pre_ref,
    post_ref,
    shift_ref,
    spike_ref,
    unit_ref,
    value_taps_ref,
    gate_taps_ref,
    out_ref,
    whole,
    x_all,
    mid_all,
    sums,
    from_partner,
    pair_sums,
    passing,
    passed,
    from_chips,
    down_from_partner,
    down_pair_sums,
    down_passing,
    down_passed,
    down_from_chips,
    down_sums,
    normed,
    hidden,
    raised,
    narrow,
    pre_gain,
    post_gain,
    shift_row,
    spike_turned,
    unit_row,
    value_taps,
    gate_taps,
    own_sem,
    send_sem,
    recv_sem,
    tp_send,
    tp_recv,
):
    f32, bf16 = jnp.float32, jnp.bfloat16
    tp = lax.axis_index("tp")
    chip, core = tp // 2, lax.rem(tp, 2)
    partner = chip * 2 + (1 - core)

    def peer(d):
        return lax.rem(chip + 4 + d, 4) * 2 + core

    barrier = pltpu.get_barrier_semaphore()
    for axis in ("y", "z"):
        for sign in (1, -1):
            pl.semaphore_signal(
                barrier, inc=1, device_id=neighbour(axis, sign), device_id_type=MESH
            )
    for other in (peer(1), peer(3), partner):
        pl.semaphore_signal(barrier, inc=1, device_id={"tp": other}, device_id_type=MESH)
    mine = pl.ds(pl.multiple_of(lax.axis_index("fs") * ROWS, ROWS), ROWS)
    pairs = (
        (query_ref, narrow.at[0], 0),
        (key_ref, narrow.at[1], 0),
        (forget_ref, narrow.at[2], 0),
        (content_ref, whole.at[mine, pl.ds(128, 128)], 1),
        (switch_ref, whole.at[mine, pl.ds(256, 128)], 1),
        (mix_ref, whole.at[mine, pl.ds(512, 128)], 2),
        (value_ref, whole.at[mine, pl.ds(640, 512)], 3),
        (gate_ref, whole.at[mine, pl.ds(1152, 512)], 3),
        (down_ref, whole.at[mine, pl.ds(1664, 512)], 3),
        (x_ref, x_all.at[tp], 4),
        (pre_ref, pre_gain, 5),
        (post_ref, post_gain, 6),
        (shift_ref, shift_row, 7),
        (spike_ref, spike_turned, 8),
        (unit_ref, unit_row, 9),
        (value_taps_ref, value_taps, 10),
        (gate_taps_ref, gate_taps, 11),
    )
    own = [pltpu.make_async_copy(a, b, own_sem.at[i]) for a, b, i in pairs]
    for one in own:
        one.start()

    def landed(at, number):
        pltpu.make_async_copy(at, at, own_sem.at[number]).wait()

    landed(narrow, 0)
    whole[mine, 0:128] = jnp.concatenate((narrow[0], narrow[1]), axis=1)
    whole[mine, 384:512] = jnp.concatenate((narrow[2], jnp.zeros_like(narrow[2])), axis=1)
    landed(whole.at[mine, pl.ds(128, 256)], 1)
    landed(whole.at[mine, pl.ds(640, 1536)], 3)
    own[5].wait()
    own[9].wait()
    pl.semaphore_wait(barrier, 7)

    def copy_of(m, step):
        o = dict(m["o"])
        o[m["axis"]] = o[m["axis"]] + step * m["sign"]
        row = pl.multiple_of(block_of(o) * ROWS + m["r0"], 16)
        at = whole.at[pl.ds(row, m["rn"]), pl.ds(m["lo"], m["hi"] - m["lo"])]
        return pltpu.make_async_remote_copy(
            src_ref=at,
            dst_ref=at,
            send_sem=send_sem.at[0],
            recv_sem=recv_sem.at[m["sem"]],
            device_id=neighbour(m["axis"], m["sign"]),
            device_id_type=MESH,
        )

    seen, waiting, ahead = set(), list(order), [AHEAD_FIRST]

    def arrived(m):
        if m["sem"] not in seen:
            seen.add(m["sem"])
            at = whole.at[pl.ds(0, m["together"]), pl.ds(m["lo"], m["hi"] - m["lo"])]
            pltpu.make_async_remote_copy(
                src_ref=at,
                dst_ref=at,
                send_sem=send_sem.at[0],
                recv_sem=recv_sem.at[m["sem"]],
                device_id=neighbour(m["axis"], m["sign"]),
                device_id_type=MESH,
            ).wait_recv()

    def pump(until):
        later = []
        for m in waiting:
            if m["start"] > until + ahead[0] or m["ready"] > until:
                later.append(m)
                continue
            for d in m["deps"]:
                arrived(d)
            copy_of(m, 0).start()
        waiting[:] = later

    def class_arrived(cls):
        mine_of = sorted((m for m in order if m["cls"] == cls), key=lambda m: m["arrive"])
        for m in mine_of:
            if m["final"]:
                pump(m["arrive"])
                arrived(m)
        return mine_of[-1]["arrive"]

    def from_depth(cls, dz):
        came = [m for m in order if m["cls"] == cls and m["dz"] == dz]
        for m in sorted(came, key=lambda m: m["arrive"]):
            if m["final"]:
                pump(m["arrive"])
                arrived(m)

    def tp_copy(src, dst, number, to):
        return pltpu.make_async_remote_copy(
            src_ref=src,
            dst_ref=dst,
            send_sem=tp_send.at[number // 10],
            recv_sem=tp_recv.at[number],
            device_id={"tp": to},
            device_id_type=MESH,
        )

    def begin(copy):
        copy.start()

    right, left = peer(1), peer(3)
    low, high = pl.ds(0, LENGTH // 2), pl.ds(LENGTH // 2, LENGTH // 2)

    def move(buf, owner, rows, number, to):
        at = buf.at[owner, rows]
        return tp_copy(at, at, number, to)

    def share(buf, base, clock):
        begin(move(buf, tp, low, base, right))
        begin(move(buf, tp, high, base + 1, left))
        begin(move(buf, tp, high, base + 2, right))
        begin(move(buf, tp, low, base + 3, left))
        begin(tp_copy(buf.at[tp], buf.at[tp], base + 6, partner))
        clock(1.5)
        clock(1.5)
        move(buf, left, low, base, right).wait_recv()
        begin(move(buf, left, low, base + 4, right))
        move(buf, right, high, base + 1, left).wait_recv()
        begin(move(buf, right, high, base + 5, left))
        clock(1.0)
        move(buf, left, high, base + 2, right).wait_recv()
        begin(tp_copy(buf.at[left], buf.at[left], base + 7, partner))
        move(buf, right, low, base + 3, left).wait_recv()
        begin(tp_copy(buf.at[right], buf.at[right], base + 8, partner))
        clock(1.0)
        clock(1.0)
        far = peer(2)
        move(buf, far, low, base + 4, right).wait_recv()
        move(buf, far, high, base + 5, left).wait_recv()
        begin(tp_copy(buf.at[far], buf.at[far], base + 9, partner))
        clock(1.0)
        for k, d in enumerate((0, 3, 1, 2)):
            came = buf.at[lax.rem(chip + d, 4) * 2 + (1 - core)]
            tp_copy(came, came, base + 6 + k, partner).wait_recv()

    def summed(product, sums, got, paired, through, joined, chips, base, clock):
        def products(d):
            there = lax.rem(chip + d, 4) * 2
            sums[there + 1 - core] = product(there + 1 - core).astype(bf16)
            sums[there + core] = product(there + core).astype(bf16)
            return tp_copy(sums.at[there + 1 - core], got.at[d], base + d, partner)

        def pair(d):
            there = lax.rem(chip + d, 4) * 2 + core
            tp_copy(sums.at[there], got.at[d], base + d, partner).wait_recv()
            paired[d - 1] = (sums[there].astype(f32) + got[d].astype(f32)).astype(bf16)

        for d in (2, 1, 3):
            begin(products(d))
            clock(0.25)
        clock(0.5)
        pair(2)
        ready = products(0)
        begin(tp_copy(paired.at[1, low], through.at[0], base + 4, right))
        begin(tp_copy(paired.at[1, high], through.at[1], base + 5, left))
        begin(ready)
        clock(0.5)
        pair(1)
        pair(3)
        begin(tp_copy(paired.at[0, high], chips.at[0, high], base + 6, right))
        tp_copy(sums.at[tp], got.at[0], base, partner).wait_recv()
        total = sums[tp].astype(f32) + got[0].astype(f32)
        begin(tp_copy(paired.at[2, low], chips.at[1, low], base + 7, left))
        clock(1.2)
        clock(1.2)
        tp_copy(through.at[0], through.at[0], base + 4, right).wait_recv()
        half = LENGTH // 2
        joined[0] = (paired[0, 0:half].astype(f32) + through[0].astype(f32)).astype(bf16)
        tp_copy(through.at[1], through.at[1], base + 5, left).wait_recv()
        joined[1] = (paired[2, half:].astype(f32) + through[1].astype(f32)).astype(bf16)
        begin(tp_copy(joined.at[0], chips.at[0, low], base + 8, right))
        begin(tp_copy(joined.at[1], chips.at[1, high], base + 9, left))
        clock(1.3)
        clock(1.3)
        tp_copy(chips.at[0, high], chips.at[0, high], base + 6, right).wait_recv()
        tp_copy(chips.at[1, low], chips.at[1, low], base + 7, left).wait_recv()
        tp_copy(chips.at[0, low], chips.at[0, low], base + 8, right).wait_recv()
        tp_copy(chips.at[1, high], chips.at[1, high], base + 9, left).wait_recv()
        return total + chips[0].astype(f32) + chips[1].astype(f32)

    ticks = [0.5]

    def tick(step):
        ticks[0] = ticks[0] + PACE * step
        pump(ticks[0])

    def still(step):
        del step

    share(x_all, 0, tick)
    for one in own[10:]:
        one.wait()
    rows_norm(x_all, pre_gain, normed)
    ticks[0] = class_arrived(0)
    ahead[0] = AHEAD
    pump(ticks[0])

    first = jnp.dot(normed[...], whole[:, 0:256], preferred_element_type=f32)
    second = jnp.dot(normed[...], whole[:, 256:512], preferred_element_type=f32)
    tick(0.7)
    rounded = first.astype(bf16).astype(f32)
    query = rounded[:, 0:64] * HEAD_K ** (-0.5)
    key = rounded[:, 64:128]
    value = rounded[:, 128:256]
    gate = second[:, 0:128].astype(bf16).astype(f32)
    forget = second[:, 128:192] + shift_row[...]
    decay = -(jnp.maximum(-forget, 0.0) + jnp.log1p(jnp.exp(-jnp.abs(forget)))) / 16.0
    decay = decay + spike_turned[...].T
    unit = unit_row[...].astype(f32)
    for piece in attention_pieces(
        query, key, value, gate, decay, unit, lambda a, s: pltpu.roll(a, s, 0)
    ):
        tick(T_PIECE)
        gated = piece

    def mix_part(t):
        rows = pl.ds(pl.multiple_of(t * COLS, COLS), COLS)
        return lax.dot_general(
            gated, whole[rows, 512:640], (((1,), (1,)), ((), ())), preferred_element_type=f32
        )

    total = summed(
        mix_part, sums, from_partner, pair_sums, passing, passed, from_chips, 10, tick
    )
    mix = total.astype(bf16)
    mid_all[tp] = (x_all[tp].astype(f32) + mix.astype(f32)).astype(bf16)
    share(mid_all, 20, tick)
    rows_norm(mid_all, post_gain, normed)
    last_of = {}
    for m in order:
        if m["cls"] == 1:
            last_of[m["dz"]] = max(last_of.get(m["dz"], 0.0), m["arrive"])
    by_arrival = sorted(last_of, key=last_of.get)
    for dz in by_arrival:
        from_depth(1, dz)
        z = lax.rem(lax.axis_index("fs") // 4 + 16 - dz, 8)
        deep = pl.ds(pl.multiple_of(z * 256, 256), 256)
        for at in (0, 512):
            part = jnp.dot(
                normed[:, deep], whole[deep, 640 + at : 1152 + at], preferred_element_type=f32
            )
            if dz == by_arrival[0]:
                raised[:, at : at + 512] = part
            else:
                raised[:, at : at + 512] = raised[:, at : at + 512] + part
    class_arrived(1)
    pump(1e9)

    for block in range(4):
        at = block * 128
        cols = slice(at, at + 128)
        up_value = raised[:, at : at + 128]
        up_gate = raised[:, 512 + at : 640 + at]
        conv_value = short_conv(up_value.astype(bf16).astype(f32), value_taps[:, cols].astype(f32))
        conv_gate = short_conv(up_gate.astype(bf16).astype(f32), gate_taps[:, cols].astype(f32))
        cube = conv_gate + 0.044715 * (conv_gate * conv_gate * conv_gate)
        gelu = conv_gate * (0.5 * (1.0 + jnp.tanh(GELU * cube)))
        hidden[:, cols] = (conv_value * gelu).astype(bf16)

    def down_part(t):
        rows = pl.ds(pl.multiple_of(t * COLS, COLS), COLS)
        return lax.dot_general(
            hidden[...], whole[rows, 1664:2176], (((1,), (1,)), ((), ())), preferred_element_type=f32
        )

    total = summed(
        down_part,
        down_sums,
        down_from_partner,
        down_pair_sums,
        down_passing,
        down_passed,
        down_from_chips,
        30,
        still,
    )
    out_ref[...] = (mid_all[tp].astype(f32) + total.astype(bf16).astype(f32)).astype(bf16)

    seven = x_all.at[pl.ds(0, 7)]
    for group in range(4):
        tp_copy(seven, seven, group * 10, partner).wait_send()
    rest = whole.at[pl.ds(0, 31 * ROWS)]
    pltpu.make_async_remote_copy(
        src_ref=rest,
        dst_ref=rest,
        send_sem=send_sem.at[0],
        recv_sem=recv_sem.at[0],
        device_id=neighbour("y", 1),
        device_id_type=MESH,
    ).wait_send()


T_PIECE = 0.5
AHEAD_FIRST = 1.0
AHEAD = 3.0
PACE = 1.3


def shards(
    incoming_features,
    attend_prenormal_scale,
    probe_matrix,
    lookup_matrix,
    content_matrix,
    forgetting_matrix,
    result_switch_matrix,
    forgetting_shift,
    spike_forget_logarithm,
    attend_unit_scale,
    attend_result_matrix,
    perceptron_scale,
    content_expand_matrix,
    switch_expand_matrix,
    content_kernel,
    switch_kernel,
    contract_matrix,
):
    order = plan(PARTS, 46.6e3, 1.8, 0.02)
    count = 1 + max(m["sem"] for m in order)
    block = (LENGTH, COLS)
    dma = pltpu.SemaphoreType.DMA
    vmem = pl.BlockSpec(memory_space=pltpu.VMEM)
    hbm = pl.BlockSpec(memory_space=pltpu.HBM)
    bf16 = jnp.bfloat16
    return pl.pallas_call(
        functools.partial(layer_kernel, order),
        out_shape=jax.ShapeDtypeStruct(block, bf16),
        in_specs=[hbm] * 17,
        out_specs=vmem,
        scratch_shapes=[
            pltpu.VMEM((32 * ROWS, WIDTH), bf16),
            pltpu.VMEM((GROUP, *block), bf16),
            pltpu.VMEM((GROUP, *block), bf16),
            pltpu.VMEM((GROUP, *block), bf16),
            pltpu.VMEM((4, *block), bf16),
            pltpu.VMEM((3, *block), bf16),
            pltpu.VMEM((2, LENGTH // 2, COLS), bf16),
            pltpu.VMEM((2, LENGTH // 2, COLS), bf16),
            pltpu.VMEM((2, *block), bf16),
            pltpu.VMEM((4, *block), bf16),
            pltpu.VMEM((3, *block), bf16),
            pltpu.VMEM((2, LENGTH // 2, COLS), bf16),
            pltpu.VMEM((2, LENGTH // 2, COLS), bf16),
            pltpu.VMEM((2, *block), bf16),
            pltpu.VMEM((GROUP, *block), bf16),
            pltpu.VMEM((LENGTH, GROUP * COLS), bf16),
            pltpu.VMEM((LENGTH, 512), bf16),
            pltpu.VMEM((LENGTH, 1024), jnp.float32),
            pltpu.VMEM((3, ROWS, 64), bf16),
            pltpu.VMEM((2048,), bf16),
            pltpu.VMEM((2048,), bf16),
            pltpu.VMEM((1, 64), jnp.float32),
            pltpu.VMEM((64, LENGTH), jnp.float32),
            pltpu.VMEM((1, 128), bf16),
            pltpu.VMEM((3, 512), bf16),
            pltpu.VMEM((3, 512), bf16),
            dma((12,)),
            dma((1,)),
            dma((count,)),
            dma((4,)),
            dma((40,)),
        ],
        compiler_params=pltpu.CompilerParams(
            collective_id=0, has_side_effects=True, vmem_limit_bytes=67043328
        ),
    )(
        probe_matrix,
        lookup_matrix,
        content_matrix,
        result_switch_matrix,
        forgetting_matrix,
        attend_result_matrix.T,
        content_expand_matrix,
        switch_expand_matrix,
        contract_matrix.T,
        incoming_features,
        attend_prenormal_scale,
        perceptron_scale,
        forgetting_shift[None],
        spike_forget_logarithm.T,
        attend_unit_scale[None],
        content_kernel,
        switch_kernel,
    )


def solution(mesh):
    placed = (
        P(("rep", "fs"), "tp"),
        P(),
        P("fs", "tp"),
        P("fs", "tp"),
        P("fs", "tp"),
        P("fs", "tp"),
        P("fs", "tp"),
        P("tp"),
        P(("rep", "fs"), "tp"),
        P("tp"),
        P("tp", "fs"),
        P(),
        P("fs", "tp"),
        P("fs", "tp"),
        P(None, "tp"),
        P(None, "tp"),
        P("tp", "fs"),
    )
    return jax.shard_map(
        shards, mesh=mesh, in_specs=placed, out_specs=P(("rep", "fs"), "tp"), check_vma=False
    )
```

```python
import functools
import heapq

import jax
import jax.numpy as jnp
from jax import lax
from jax.experimental import pallas as pl
from jax.experimental.pallas import tpu as pltpu
from jax.sharding import PartitionSpec as P

HEAD_K = 32
HEAD_V = 64
SUB = 16
NEVER = -1e30
norm_eps = 1e-06
MESH = pl.DeviceIdType.MESH
WIDTH = 2176
PARTS = (
    (0, "A", 0, 256),
    (0, "B", 256, 640),
    (1, "A", 640, 1280),
    (1, "B", 1280, 2176),
)
LENGTH = 192
GROUP = 8
COLS = 256
GELU = 0.7978845608028654

ROWS = 64
SIZES = {"y": 4, "z": 8}


def tree_messages(cls, tree, lo, hi):
    first, second = ("y", "z") if tree == "A" else ("z", "y")
    msgs = []

    def chain(axis, base, deps, stage):
        n = SIZES[axis]
        made = []
        for sign in (1, -1):
            d, s = deps, stage
            for k in range(1, n // 2 + 1):
                o = dict(base)
                o[axis] = sign * (k - 1)
                r0, rn = 0, ROWS
                if k == n // 2:
                    rn = ROWS // 2
                    r0 = 0 if sign > 0 else rn
                m = dict(
                    cls=cls, lo=lo, hi=hi, axis=axis, sign=sign, o=o, r0=r0, rn=rn, deps=d, off=sign * k, stage=s
                )
                msgs.append(m)
                made.append(m)
                d, s = (m,), s + 1
        return made

    made = chain(first, {"y": 0, "z": 0}, (), 0)
    chain(second, {"y": 0, "z": 0}, (), 0)
    far = SIZES[first] // 2
    for m in made:
        if abs(m["off"]) < far:
            chain(second, {first: m["off"], second: 0}, (m,), m["stage"] + 1)
    halves = tuple(m for m in made if abs(m["off"]) == far)
    chain(second, {first: far, second: 0}, halves, halves[0]["stage"] + 1)
    return msgs


def plan(parts, rate, lat, each):
    msgs = []
    for p in parts:
        msgs += tree_messages(*p)
    kids = {}
    parents = {id(d) for m in msgs for d in m["deps"]}
    twins = {}
    for m in msgs:
        m["dz"] = m["o"]["z"] + (m["sign"] if m["axis"] == "z" else 0)
        m["dz"] = 4 if abs(m["dz"]) == 4 else m["dz"]
        across = m["o"]["y" if m["axis"] == "z" else "z"]
        if id(m) in parents:
            m["key"] = (m["lo"], m["axis"], across, abs(m["off"]))
        else:
            m["key"] = (m["lo"], m["axis"], m["dz"], "leaf")
        twins.setdefault(m["key"], []).append(m)
    for m in msgs:
        keys = dict.fromkeys(d["key"] for d in m["deps"])
        m["deps"] = tuple(t for k in keys for t in twins[k])
    for i, m in enumerate(msgs):
        m["id"] = i
    for m in msgs:
        m["bytes"] = m["rn"] * (m["hi"] - m["lo"]) * 2
        m["need"] = len(m["deps"])
        for d in m["deps"]:
            kids.setdefault(d["id"], []).append(m)
    depth = {}

    def depth_of(m):
        if m["id"] not in depth:
            depth[m["id"]] = 1 + max((depth_of(k) for k in kids.get(m["id"], ())), default=0)
        return depth[m["id"]]

    for i, members in enumerate(twins.values()):
        for m in members:
            m["sem"] = i
            m["together"] = sum(k["rn"] for k in members)
    free = {(a, s): 0.0 for a in "yz" for s in (1, -1)}
    avail = {k: [] for k in free}
    events = [(0.0, 0, m["id"]) for m in msgs if not m["deps"]]
    heapq.heapify(events)
    order = []
    while events:
        t = events[0][0]
        while events and events[0][0] <= t + 1e-9:
            _, kind, i = heapq.heappop(events)
            if kind == 0:
                m = msgs[i]
                m["ready"] = t
                heapq.heappush(avail[(m["axis"], m["sign"])], (m["cls"], -depth_of(m), i))
        for link, queue in avail.items():
            if queue and free[link] <= t + 1e-9:
                m = msgs[heapq.heappop(queue)[2]]
                m["start"] = t
                free[link] = t + m["bytes"] / rate + each
                m["arrive"] = free[link] + lat
                order.append(m)
                heapq.heappush(events, (free[link], 1, 0))
                for k in kids.get(m["id"], ()):
                    k["need"] -= 1
                    if k["need"] == 0:
                        heapq.heappush(events, (m["arrive"], 0, k["id"]))
    for members in twins.values():
        last = max(members, key=lambda m: m["arrive"])
        for m in members:
            m["final"] = m is last
    return order


def neighbour(axis, sign):
    rep, fs = lax.axis_index("rep"), lax.axis_index("fs")
    y, z = lax.rem(fs, 4), rep * 8 + fs // 4
    if axis == "y":
        y = lax.rem(y + 4 + sign, 4)
    else:
        z = lax.rem(z + 16 + sign, 16)
    return {"rep": z // 8, "fs": lax.rem(z, 8) * 4 + y}


def block_of(o):
    fs = lax.axis_index("fs")
    y, z = lax.rem(fs, 4), fs // 4
    y = lax.rem(y + 8 - o["y"], 4)
    z = lax.rem(z + 16 - o["z"], 8)
    return z * 4 + y


def attention_pieces(q, k, v, g, ld, unit, roll):
    length = q.shape[0]
    blocks = length // SUB
    exact = lax.Precision.HIGHEST
    row = lax.broadcasted_iota(jnp.int32, (length, 64), 0) % SUB
    c = ld
    shift = 1
    while shift < SUB:
        c = c + jnp.where(row >= shift, roll(c, shift), 0.0)
        shift *= 2
    key_head = lax.broadcasted_iota(jnp.int32, (64, 128), 0) // HEAD_K
    value_head = lax.broadcasted_iota(jnp.int32, (64, 128), 1) // HEAD_V
    spread = jnp.where(key_head == value_head, 1.0, 0.0)
    c3 = c.reshape(blocks, SUB, 64)
    total = c3[:, SUB - 1 : SUB, :]
    k_end = (k.reshape(blocks, SUB, 64) * jnp.exp(total - c3))
    q_in = q * jnp.exp(c)
    v3 = v.reshape(blocks, SUB, 128)
    fade = jnp.exp(total)
    q3 = q_in.reshape(blocks, SUB, 64)
    own_head = (
        lax.broadcasted_iota(jnp.int32, (128, 64), 0) // HEAD_V
        == lax.broadcasted_iota(jnp.int32, (128, 64), 1) // HEAD_K
    )
    yield None
    out = jnp.zeros((length, 128), jnp.float32)
    for j in range(SUB):
        if j == 0:
            pairs, values = q * k, v
        else:
            differ = jnp.where(row >= j, c - roll(c, j), NEVER)
            pairs, values = q * roll(k, j) * jnp.exp(differ), roll(v, j)
        scores = jnp.dot(pairs, spread, precision=exact, preferred_element_type=jnp.float32)
        out = out + scores * values
        if j % 4 == 3:
            yield None
    state = None
    carried = [jnp.zeros((SUB, 128), jnp.float32)]
    for i in range(blocks):
        if state is not None:
            carried.append(
                lax.dot_general(
                    q3[i], state, (((1,), (1,)), ((), ())), precision=exact,
                    preferred_element_type=jnp.float32,
                )
            )
        if i < blocks - 1:
            update = lax.dot_general(
                v3[i], k_end[i], (((0,), (0,)), ((), ())), precision=exact,
                preferred_element_type=jnp.float32,
            )
            update = jnp.where(own_head, update, 0.0)
            state = update if state is None else state * fade[i] + update
        if i % 4 == 3:
            yield None
    out = out + jnp.concatenate(carried, axis=0)
    same = jnp.where(
        lax.broadcasted_iota(jnp.int32, (128, 128), 0) // HEAD_V
        == lax.broadcasted_iota(jnp.int32, (128, 128), 1) // HEAD_V,
        1.0 / HEAD_V,
        0.0,
    )
    mean = jnp.dot(out * out, same, precision=exact, preferred_element_type=jnp.float32)
    out = out * lax.rsqrt(mean + norm_eps) * unit * (g / (1.0 + jnp.exp(-g)))
    yield out.astype(jnp.bfloat16)


def rows_norm(blocks, gain_ref, out):
    total = jnp.zeros((LENGTH, COLS), jnp.float32)
    for t in range(GROUP):
        one = blocks[t].astype(jnp.float32)
        total = total + one * one
    mean = jnp.sum(total, axis=1, keepdims=True) * (1.0 / (GROUP * COLS))
    scale = lax.rsqrt(mean + norm_eps)
    for t in range(GROUP):
        at = slice(t * COLS, (t + 1) * COLS)
        gain = gain_ref[at].astype(jnp.float32).reshape(1, COLS)
        out[:, at] = (blocks[t].astype(jnp.float32) * scale * gain).astype(jnp.bfloat16)


def short_conv(tokens, taps):
    row = lax.broadcasted_iota(jnp.int32, tokens.shape, 0)
    one = jnp.where(row >= 1, pltpu.roll(tokens, 1, 0), 0.0)
    two = jnp.where(row >= 2, pltpu.roll(tokens, 2, 0), 0.0)
    return two * taps[0:1] + one * taps[1:2] + tokens * taps[2:3]


def layer_kernel(
    order,
    query_ref,
    key_ref,
    content_ref,
    switch_ref,
    forget_ref,
    mix_ref,
    value_ref,
    gate_ref,
    down_ref,
    x_ref,
    pre_ref,
    post_ref,
    shift_ref,
    spike_ref,
    unit_ref,
    value_taps_ref,
    gate_taps_ref,
    out_ref,
    whole,
    x_all,
    mid_all,
    sums,
    from_partner,
    pair_sums,
    passing,
    passed,
    from_chips,
    down_from_partner,
    down_pair_sums,
    down_passing,
    down_passed,
    down_from_chips,
    down_sums,
    normed,
    hidden,
    raised,
    narrow,
    pre_gain,
    post_gain,
    shift_row,
    spike_turned,
    unit_row,
    value_taps,
    gate_taps,
    own_sem,
    send_sem,
    recv_sem,
    tp_send,
    tp_recv,
):
    f32, bf16 = jnp.float32, jnp.bfloat16
    tp = lax.axis_index("tp")
    chip, core = tp // 2, lax.rem(tp, 2)
    partner = chip * 2 + (1 - core)

    def peer(d):
        return lax.rem(chip + 4 + d, 4) * 2 + core

    barrier = pltpu.get_barrier_semaphore()
    for axis in ("y", "z"):
        for sign in (1, -1):
            pl.semaphore_signal(
                barrier, inc=1, device_id=neighbour(axis, sign), device_id_type=MESH
            )
    for other in (peer(1), peer(3), partner):
        pl.semaphore_signal(barrier, inc=1, device_id={"tp": other}, device_id_type=MESH)
    mine = pl.ds(pl.multiple_of(lax.axis_index("fs") * ROWS, ROWS), ROWS)
    pairs = (
        (query_ref, narrow.at[0], 0),
        (key_ref, narrow.at[1], 0),
        (forget_ref, narrow.at[2], 0),
        (content_ref, whole.at[mine, pl.ds(128, 128)], 1),
        (switch_ref, whole.at[mine, pl.ds(256, 128)], 1),
        (mix_ref, whole.at[mine, pl.ds(512, 128)], 2),
        (value_ref, whole.at[mine, pl.ds(640, 512)], 3),
        (gate_ref, whole.at[mine, pl.ds(1152, 512)], 3),
        (down_ref, whole.at[mine, pl.ds(1664, 512)], 3),
        (x_ref, x_all.at[tp], 4),
        (pre_ref, pre_gain, 5),
        (post_ref, post_gain, 6),
        (shift_ref, shift_row, 7),
        (spike_ref, spike_turned, 8),
        (unit_ref, unit_row, 9),
        (value_taps_ref, value_taps, 10),
        (gate_taps_ref, gate_taps, 11),
    )
    own = [pltpu.make_async_copy(a, b, own_sem.at[i]) for a, b, i in pairs]
    for one in own:
        one.start()

    def landed(at, number):
        pltpu.make_async_copy(at, at, own_sem.at[number]).wait()

    landed(narrow, 0)
    whole[mine, 0:128] = jnp.concatenate((narrow[0], narrow[1]), axis=1)
    whole[mine, 384:512] = jnp.concatenate((narrow[2], jnp.zeros_like(narrow[2])), axis=1)
    landed(whole.at[mine, pl.ds(128, 256)], 1)
    own[5].wait()
    pl.semaphore_wait(barrier, 7)

    def copy_of(m, step):
        o = dict(m["o"])
        o[m["axis"]] = o[m["axis"]] + step * m["sign"]
        row = pl.multiple_of(block_of(o) * ROWS + m["r0"], 16)
        at = whole.at[pl.ds(row, m["rn"]), pl.ds(m["lo"], m["hi"] - m["lo"])]
        return pltpu.make_async_remote_copy(
            src_ref=at,
            dst_ref=at,
            send_sem=send_sem.at[0],
            recv_sem=recv_sem.at[m["sem"]],
            device_id=neighbour(m["axis"], m["sign"]),
            device_id_type=MESH,
        )

    seen, waiting, ahead = set(), list(order), [AHEAD_FIRST]

    def arrived(m):
        if m["sem"] not in seen:
            seen.add(m["sem"])
            at = whole.at[pl.ds(0, m["together"]), pl.ds(m["lo"], m["hi"] - m["lo"])]
            pltpu.make_async_remote_copy(
                src_ref=at,
                dst_ref=at,
                send_sem=send_sem.at[0],
                recv_sem=recv_sem.at[m["sem"]],
                device_id=neighbour(m["axis"], m["sign"]),
                device_id_type=MESH,
            ).wait_recv()

    def pump(until):
        later = []
        for m in waiting:
            if m["start"] > until + ahead[0] or m["ready"] > until:
                later.append(m)
                continue
            for d in m["deps"]:
                arrived(d)
            copy_of(m, 0).start()
        waiting[:] = later

    def class_arrived(cls):
        mine_of = sorted((m for m in order if m["cls"] == cls), key=lambda m: m["arrive"])
        for m in mine_of:
            if m["final"]:
                pump(m["arrive"])
                arrived(m)
        return mine_of[-1]["arrive"]

    def from_depth(cls, dz):
        came = [m for m in order if m["cls"] == cls and m["dz"] == dz]
        for m in sorted(came, key=lambda m: m["arrive"]):
            if m["final"]:
                pump(m["arrive"])
                arrived(m)

    def tp_copy(src, dst, number, to):
        return pltpu.make_async_remote_copy(
            src_ref=src,
            dst_ref=dst,
            send_sem=tp_send.at[number // 10],
            recv_sem=tp_recv.at[number // 10 * 7 + number % 10],
            device_id={"tp": to},
            device_id_type=MESH,
        )

    def begin(copy):
        copy.start()

    right, left = peer(1), peer(3)
    low, high = pl.ds(0, LENGTH // 2), pl.ds(LENGTH // 2, LENGTH // 2)

    def move(buf, owner, rows, number, to):
        at = buf.at[owner, rows]
        return tp_copy(at, at, number, to)

    def share(buf, base, clock):
        begin(move(buf, tp, low, base, right))
        begin(move(buf, tp, high, base + 1, left))
        begin(move(buf, tp, high, base + 2, right))
        begin(move(buf, tp, low, base + 3, left))
        begin(tp_copy(buf.at[tp], buf.at[tp], base + 6, partner))
        clock(1.5)
        clock(1.5)
        move(buf, left, low, base, right).wait_recv()
        begin(move(buf, left, low, base + 4, right))
        move(buf, right, high, base + 1, left).wait_recv()
        begin(move(buf, right, high, base + 5, left))
        clock(1.0)
        move(buf, left, high, base + 2, right).wait_recv()
        begin(tp_copy(buf.at[left], buf.at[left], base + 6, partner))
        move(buf, right, low, base + 3, left).wait_recv()
        begin(tp_copy(buf.at[right], buf.at[right], base + 6, partner))
        clock(1.0)
        clock(1.0)
        far = peer(2)
        move(buf, far, low, base + 4, right).wait_recv()
        move(buf, far, high, base + 5, left).wait_recv()
        begin(tp_copy(buf.at[far], buf.at[far], base + 6, partner))
        clock(1.0)
        came = buf.at[pl.ds(0, 4)]
        tp_copy(came, came, base + 6, partner).wait_recv()

    def summed(product, sums, got, paired, through, joined, chips, base, clock):
        def products(d):
            there = lax.rem(chip + d, 4) * 2
            sums[there + 1 - core] = product(there + 1 - core).astype(bf16)
            sums[there + core] = product(there + core).astype(bf16)
            return tp_copy(sums.at[there + 1 - core], got.at[d], base + d, partner)

        def pair(d):
            there = lax.rem(chip + d, 4) * 2 + core
            tp_copy(sums.at[there], got.at[d], base + d, partner).wait_recv()
            paired[d - 1] = (sums[there].astype(f32) + got[d].astype(f32)).astype(bf16)

        for d in (2, 1, 3, 0):
            begin(products(d))
            clock(0.25)
        clock(0.25)
        pair(2)
        begin(tp_copy(paired.at[1, low], through.at[0], base + 4, right))
        begin(tp_copy(paired.at[1, high], through.at[1], base + 5, left))
        clock(0.5)
        pair(1)
        pair(3)
        begin(tp_copy(paired.at[0, high], chips.at[0, high], base + 6, right))
        tp_copy(sums.at[tp], got.at[0], base, partner).wait_recv()
        total = sums[tp].astype(f32) + got[0].astype(f32)
        begin(tp_copy(paired.at[2, low], chips.at[1, low], base + 6, left))
        clock(1.2)
        clock(1.2)
        tp_copy(through.at[0], through.at[0], base + 4, right).wait_recv()
        half = LENGTH // 2
        joined[0] = (paired[0, 0:half].astype(f32) + through[0].astype(f32)).astype(bf16)
        tp_copy(through.at[1], through.at[1], base + 5, left).wait_recv()
        joined[1] = (paired[2, half:].astype(f32) + through[1].astype(f32)).astype(bf16)
        begin(tp_copy(joined.at[0], chips.at[0, low], base + 6, right))
        begin(tp_copy(joined.at[1], chips.at[1, high], base + 6, left))
        clock(1.3)
        clock(1.3)
        tp_copy(chips, chips, base + 6, right).wait_recv()
        return total + chips[0].astype(f32) + chips[1].astype(f32)

    ticks = [0.5]

    def tick(step):
        ticks[0] = ticks[0] + PACE * step
        pump(ticks[0])

    def still(step):
        del step

    pump(0.0)
    landed(whole.at[mine, pl.ds(640, 1536)], 3)
    own[9].wait()
    share(x_all, 0, tick)
    for one in own[10:]:
        one.wait()
    rows_norm(x_all, pre_gain, normed)
    ticks[0] = class_arrived(0)
    ahead[0] = AHEAD
    pump(ticks[0])

    first = jnp.dot(normed[...], whole[:, 0:256], preferred_element_type=f32)
    second = jnp.dot(normed[...], whole[:, 256:512], preferred_element_type=f32)
    tick(0.7)
    rounded = first.astype(bf16).astype(f32)
    query = rounded[:, 0:64] * HEAD_K ** (-0.5)
    key = rounded[:, 64:128]
    value = rounded[:, 128:256]
    gate = second[:, 0:128].astype(bf16).astype(f32)
    forget = second[:, 128:192] + shift_row[...]
    decay = -(jnp.maximum(-forget, 0.0) + jnp.log1p(jnp.exp(-jnp.abs(forget)))) / 16.0
    decay = decay + spike_turned[...].T
    unit = unit_row[...].astype(f32)
    for piece in attention_pieces(
        query, key, value, gate, decay, unit, lambda a, s: pltpu.roll(a, s, 0)
    ):
        tick(T_PIECE)
        gated = piece

    def mix_part(t):
        rows = pl.ds(pl.multiple_of(t * COLS, COLS), COLS)
        return lax.dot_general(
            gated, whole[rows, 512:640], (((1,), (1,)), ((), ())), preferred_element_type=f32
        )

    total = summed(
        mix_part, sums, from_partner, pair_sums, passing, passed, from_chips, 10, tick
    )
    mix = total.astype(bf16)
    mid_all[tp] = (x_all[tp].astype(f32) + mix.astype(f32)).astype(bf16)
    share(mid_all, 20, tick)
    rows_norm(mid_all, post_gain, normed)
    last_of = {}
    for m in order:
        if m["cls"] == 1:
            last_of[m["dz"]] = max(last_of.get(m["dz"], 0.0), m["arrive"])
    by_arrival = sorted(last_of, key=last_of.get)
    for dz in by_arrival:
        from_depth(1, dz)
        z = lax.rem(lax.axis_index("fs") // 4 + 16 - dz, 8)
        deep = pl.ds(pl.multiple_of(z * 256, 256), 256)
        for at in (0, 512):
            part = jnp.dot(
                normed[:, deep], whole[deep, 640 + at : 1152 + at], preferred_element_type=f32
            )
            if dz == by_arrival[0]:
                raised[:, at : at + 512] = part
            else:
                raised[:, at : at + 512] = raised[:, at : at + 512] + part
    class_arrived(1)
    pump(1e9)

    for block in range(4):
        at = block * 128
        cols = slice(at, at + 128)
        up_value = raised[:, at : at + 128]
        up_gate = raised[:, 512 + at : 640 + at]
        conv_value = short_conv(up_value.astype(bf16).astype(f32), value_taps[:, cols].astype(f32))
        conv_gate = short_conv(up_gate.astype(bf16).astype(f32), gate_taps[:, cols].astype(f32))
        cube = conv_gate + 0.044715 * (conv_gate * conv_gate * conv_gate)
        gelu = conv_gate * (0.5 * (1.0 + jnp.tanh(GELU * cube)))
        hidden[:, cols] = (conv_value * gelu).astype(bf16)

    def down_part(t):
        rows = pl.ds(pl.multiple_of(t * COLS, COLS), COLS)
        return lax.dot_general(
            hidden[...], whole[rows, 1664:2176], (((1,), (1,)), ((), ())), preferred_element_type=f32
        )

    total = summed(
        down_part,
        down_sums,
        down_from_partner,
        down_pair_sums,
        down_passing,
        down_passed,
        down_from_chips,
        30,
        still,
    )
    out_ref[...] = (mid_all[tp].astype(f32) + total.astype(bf16).astype(f32)).astype(bf16)

    seven = x_all.at[pl.ds(0, 7)]
    for group in range(4):
        tp_copy(seven, seven, group * 10, partner).wait_send()
    rest = whole.at[pl.ds(0, 31 * ROWS)]
    pltpu.make_async_remote_copy(
        src_ref=rest,
        dst_ref=rest,
        send_sem=send_sem.at[0],
        recv_sem=recv_sem.at[0],
        device_id=neighbour("y", 1),
        device_id_type=MESH,
    ).wait_send()


T_PIECE = 0.5
AHEAD_FIRST = 1.0
AHEAD = 3.0
PACE = 1.4


def shards(
    incoming_features,
    attend_prenormal_scale,
    probe_matrix,
    lookup_matrix,
    content_matrix,
    forgetting_matrix,
    result_switch_matrix,
    forgetting_shift,
    spike_forget_logarithm,
    attend_unit_scale,
    attend_result_matrix,
    perceptron_scale,
    content_expand_matrix,
    switch_expand_matrix,
    content_kernel,
    switch_kernel,
    contract_matrix,
):
    order = plan(PARTS, 46.6e3, 1.8, 0.02)
    count = 1 + max(m["sem"] for m in order)
    block = (LENGTH, COLS)
    dma = pltpu.SemaphoreType.DMA
    vmem = pl.BlockSpec(memory_space=pltpu.VMEM)
    hbm = pl.BlockSpec(memory_space=pltpu.HBM)
    bf16 = jnp.bfloat16
    return pl.pallas_call(
        functools.partial(layer_kernel, order),
        out_shape=jax.ShapeDtypeStruct(block, bf16),
        in_specs=[hbm] * 17,
        out_specs=vmem,
        scratch_shapes=[
            pltpu.VMEM((32 * ROWS, WIDTH), bf16),
            pltpu.VMEM((GROUP, *block), bf16),
            pltpu.VMEM((GROUP, *block), bf16),
            pltpu.VMEM((GROUP, *block), bf16),
            pltpu.VMEM((4, *block), bf16),
            pltpu.VMEM((3, *block), bf16),
            pltpu.VMEM((2, LENGTH // 2, COLS), bf16),
            pltpu.VMEM((2, LENGTH // 2, COLS), bf16),
            pltpu.VMEM((2, *block), bf16),
            pltpu.VMEM((4, *block), bf16),
            pltpu.VMEM((3, *block), bf16),
            pltpu.VMEM((2, LENGTH // 2, COLS), bf16),
            pltpu.VMEM((2, LENGTH // 2, COLS), bf16),
            pltpu.VMEM((2, *block), bf16),
            pltpu.VMEM((GROUP, *block), bf16),
            pltpu.VMEM((LENGTH, GROUP * COLS), bf16),
            pltpu.VMEM((LENGTH, 512), bf16),
            pltpu.VMEM((LENGTH, 1024), jnp.float32),
            pltpu.VMEM((3, ROWS, 64), bf16),
            pltpu.VMEM((2048,), bf16),
            pltpu.VMEM((2048,), bf16),
            pltpu.VMEM((1, 64), jnp.float32),
            pltpu.VMEM((64, LENGTH), jnp.float32),
            pltpu.VMEM((1, 128), bf16),
            pltpu.VMEM((3, 512), bf16),
            pltpu.VMEM((3, 512), bf16),
            dma((12,)),
            dma((1,)),
            dma((count,)),
            dma((4,)),
            dma((28,)),
        ],
        compiler_params=pltpu.CompilerParams(
            collective_id=0, has_side_effects=True, vmem_limit_bytes=67043328
        ),
    )(
        probe_matrix,
        lookup_matrix,
        content_matrix,
        result_switch_matrix,
        forgetting_matrix,
        attend_result_matrix.T,
        content_expand_matrix,
        switch_expand_matrix,
        contract_matrix.T,
        incoming_features,
        attend_prenormal_scale,
        perceptron_scale,
        forgetting_shift[None],
        spike_forget_logarithm.T,
        attend_unit_scale[None],
        content_kernel,
        switch_kernel,
    )


def solution(mesh):
    placed = (
        P(("rep", "fs"), "tp"),
        P(),
        P("fs", "tp"),
        P("fs", "tp"),
        P("fs", "tp"),
        P("fs", "tp"),
        P("fs", "tp"),
        P("tp"),
        P(("rep", "fs"), "tp"),
        P("tp"),
        P("tp", "fs"),
        P(),
        P("fs", "tp"),
        P("fs", "tp"),
        P(None, "tp"),
        P(None, "tp"),
        P("tp", "fs"),
    )
    return jax.shard_map(
        shards, mesh=mesh, in_specs=placed, out_specs=P(("rep", "fs"), "tp"), check_vma=False
    )
```

```python
import functools
import heapq

import jax
import jax.numpy as jnp
from jax import lax
from jax.experimental import pallas as pl
from jax.experimental.pallas import tpu as pltpu
from jax.sharding import PartitionSpec as P

HEAD_K = 32
HEAD_V = 64
SUB = 16
NEVER = -1e30
norm_eps = 1e-06
MESH = pl.DeviceIdType.MESH
WIDTH = 2176
PARTS = (
    (0, "A", 0, 256),
    (0, "B", 256, 640),
    (1, "A", 640, 1280),
    (1, "B", 1280, 2176),
)
LENGTH = 192
GROUP = 8
COLS = 256
GELU = 0.7978845608028654

ROWS = 64
SIZES = {"y": 4, "z": 8}


def tree_messages(cls, tree, lo, hi):
    first, second = ("y", "z") if tree == "A" else ("z", "y")
    msgs = []

    def chain(axis, base, deps, stage):
        n = SIZES[axis]
        made = []
        for sign in (1, -1):
            d, s = deps, stage
            for k in range(1, n // 2 + 1):
                o = dict(base)
                o[axis] = sign * (k - 1)
                r0, rn = 0, ROWS
                if k == n // 2:
                    rn = ROWS // 2
                    r0 = 0 if sign > 0 else rn
                m = dict(
                    cls=cls, lo=lo, hi=hi, axis=axis, sign=sign, o=o, r0=r0, rn=rn, deps=d, off=sign * k, stage=s
                )
                msgs.append(m)
                made.append(m)
                d, s = (m,), s + 1
        return made

    made = chain(first, {"y": 0, "z": 0}, (), 0)
    chain(second, {"y": 0, "z": 0}, (), 0)
    far = SIZES[first] // 2
    for m in made:
        if abs(m["off"]) < far:
            chain(second, {first: m["off"], second: 0}, (m,), m["stage"] + 1)
    halves = tuple(m for m in made if abs(m["off"]) == far)
    chain(second, {first: far, second: 0}, halves, halves[0]["stage"] + 1)
    return msgs


def plan(parts, rate, lat, each):
    msgs = []
    for p in parts:
        msgs += tree_messages(*p)
    kids = {}
    parents = {id(d) for m in msgs for d in m["deps"]}
    twins = {}
    for m in msgs:
        m["dz"] = m["o"]["z"] + (m["sign"] if m["axis"] == "z" else 0)
        m["dz"] = 4 if abs(m["dz"]) == 4 else m["dz"]
        across = m["o"]["y" if m["axis"] == "z" else "z"]
        if id(m) in parents:
            m["key"] = (m["lo"], m["axis"], across, abs(m["off"]))
        else:
            m["key"] = (m["lo"], m["axis"], m["dz"], "leaf")
        twins.setdefault(m["key"], []).append(m)
    for m in msgs:
        keys = dict.fromkeys(d["key"] for d in m["deps"])
        m["deps"] = tuple(t for k in keys for t in twins[k])
    for i, m in enumerate(msgs):
        m["id"] = i
    for m in msgs:
        m["bytes"] = m["rn"] * (m["hi"] - m["lo"]) * 2
        m["need"] = len(m["deps"])
        for d in m["deps"]:
            kids.setdefault(d["id"], []).append(m)
    depth = {}

    def depth_of(m):
        if m["id"] not in depth:
            depth[m["id"]] = 1 + max((depth_of(k) for k in kids.get(m["id"], ())), default=0)
        return depth[m["id"]]

    for i, members in enumerate(twins.values()):
        for m in members:
            m["sem"] = i
            m["together"] = sum(k["rn"] for k in members)
    free = {(a, s): 0.0 for a in "yz" for s in (1, -1)}
    avail = {k: [] for k in free}
    events = [(0.0, 0, m["id"]) for m in msgs if not m["deps"]]
    heapq.heapify(events)
    order = []
    while events:
        t = events[0][0]
        while events and events[0][0] <= t + 1e-9:
            _, kind, i = heapq.heappop(events)
            if kind == 0:
                m = msgs[i]
                m["ready"] = t
                heapq.heappush(avail[(m["axis"], m["sign"])], (m["cls"], -depth_of(m), i))
        for link, queue in avail.items():
            if queue and free[link] <= t + 1e-9:
                m = msgs[heapq.heappop(queue)[2]]
                m["start"] = t
                free[link] = t + m["bytes"] / rate + each
                m["arrive"] = free[link] + lat
                order.append(m)
                heapq.heappush(events, (free[link], 1, 0))
                for k in kids.get(m["id"], ()):
                    k["need"] -= 1
                    if k["need"] == 0:
                        heapq.heappush(events, (m["arrive"], 0, k["id"]))
    for members in twins.values():
        last = max(members, key=lambda m: m["arrive"])
        for m in members:
            m["final"] = m is last
    return order


def neighbour(axis, sign):
    rep, fs = lax.axis_index("rep"), lax.axis_index("fs")
    y, z = lax.rem(fs, 4), rep * 8 + fs // 4
    if axis == "y":
        y = lax.rem(y + 4 + sign, 4)
    else:
        z = lax.rem(z + 16 + sign, 16)
    return {"rep": z // 8, "fs": lax.rem(z, 8) * 4 + y}


def block_of(o):
    fs = lax.axis_index("fs")
    y, z = lax.rem(fs, 4), fs // 4
    y = lax.rem(y + 8 - o["y"], 4)
    z = lax.rem(z + 16 - o["z"], 8)
    return z * 4 + y


def attention_pieces(q, k, v, g, ld, unit, roll):
    length = q.shape[0]
    blocks = length // SUB
    exact = lax.Precision.HIGHEST
    row = lax.broadcasted_iota(jnp.int32, (length, 64), 0) % SUB
    c = ld
    shift = 1
    while shift < SUB:
        c = c + jnp.where(row >= shift, roll(c, shift), 0.0)
        shift *= 2
    key_head = lax.broadcasted_iota(jnp.int32, (64, 128), 0) // HEAD_K
    value_head = lax.broadcasted_iota(jnp.int32, (64, 128), 1) // HEAD_V
    spread = jnp.where(key_head == value_head, 1.0, 0.0)
    c3 = c.reshape(blocks, SUB, 64)
    total = c3[:, SUB - 1 : SUB, :]
    k_end = (k.reshape(blocks, SUB, 64) * jnp.exp(total - c3))
    q_in = q * jnp.exp(c)
    v3 = v.reshape(blocks, SUB, 128)
    fade = jnp.exp(total)
    q3 = q_in.reshape(blocks, SUB, 64)
    own_head = (
        lax.broadcasted_iota(jnp.int32, (128, 64), 0) // HEAD_V
        == lax.broadcasted_iota(jnp.int32, (128, 64), 1) // HEAD_K
    )
    yield None
    out = jnp.zeros((length, 128), jnp.float32)
    for j in range(SUB):
        if j == 0:
            pairs, values = q * k, v
        else:
            differ = jnp.where(row >= j, c - roll(c, j), NEVER)
            pairs, values = q * roll(k, j) * jnp.exp(differ), roll(v, j)
        scores = jnp.dot(pairs, spread, precision=exact, preferred_element_type=jnp.float32)
        out = out + scores * values
        if j % 4 == 3:
            yield None
    state = None
    carried = [jnp.zeros((SUB, 128), jnp.float32)]
    for i in range(blocks):
        if state is not None:
            carried.append(
                lax.dot_general(
                    q3[i], state, (((1,), (1,)), ((), ())), precision=exact,
                    preferred_element_type=jnp.float32,
                )
            )
        if i < blocks - 1:
            update = lax.dot_general(
                v3[i], k_end[i], (((0,), (0,)), ((), ())), precision=exact,
                preferred_element_type=jnp.float32,
            )
            update = jnp.where(own_head, update, 0.0)
            state = update if state is None else state * fade[i] + update
        if i % 4 == 3:
            yield None
    out = out + jnp.concatenate(carried, axis=0)
    same = jnp.where(
        lax.broadcasted_iota(jnp.int32, (128, 128), 0) // HEAD_V
        == lax.broadcasted_iota(jnp.int32, (128, 128), 1) // HEAD_V,
        1.0 / HEAD_V,
        0.0,
    )
    mean = jnp.dot(out * out, same, precision=exact, preferred_element_type=jnp.float32)
    out = out * lax.rsqrt(mean + norm_eps) * unit * (g / (1.0 + jnp.exp(-g)))
    yield out.astype(jnp.bfloat16)


def rows_norm(blocks, gain_ref, out):
    total = jnp.zeros((LENGTH, COLS), jnp.float32)
    for t in range(GROUP):
        one = blocks[t].astype(jnp.float32)
        total = total + one * one
    mean = jnp.sum(total, axis=1, keepdims=True) * (1.0 / (GROUP * COLS))
    scale = lax.rsqrt(mean + norm_eps)
    for t in range(GROUP):
        at = slice(t * COLS, (t + 1) * COLS)
        gain = gain_ref[at].astype(jnp.float32).reshape(1, COLS)
        out[:, at] = (blocks[t].astype(jnp.float32) * scale * gain).astype(jnp.bfloat16)


def short_conv(tokens, taps):
    row = lax.broadcasted_iota(jnp.int32, tokens.shape, 0)
    one = jnp.where(row >= 1, pltpu.roll(tokens, 1, 0), 0.0)
    two = jnp.where(row >= 2, pltpu.roll(tokens, 2, 0), 0.0)
    return two * taps[0:1] + one * taps[1:2] + tokens * taps[2:3]


def layer_kernel(
    order,
    query_ref,
    key_ref,
    content_ref,
    switch_ref,
    forget_ref,
    mix_ref,
    value_ref,
    gate_ref,
    down_ref,
    x_ref,
    pre_ref,
    post_ref,
    shift_ref,
    spike_ref,
    unit_ref,
    value_taps_ref,
    gate_taps_ref,
    out_ref,
    whole,
    x_all,
    mid_all,
    sums,
    from_partner,
    pair_sums,
    passing,
    passed,
    from_chips,
    down_from_partner,
    down_pair_sums,
    down_passing,
    down_passed,
    down_from_chips,
    down_sums,
    normed,
    hidden,
    raised,
    narrow,
    pre_gain,
    post_gain,
    shift_row,
    spike_turned,
    unit_row,
    value_taps,
    gate_taps,
    own_sem,
    send_sem,
    recv_sem,
    tp_send,
    tp_recv,
):
    f32, bf16 = jnp.float32, jnp.bfloat16
    tp = lax.axis_index("tp")
    chip, core = tp // 2, lax.rem(tp, 2)
    partner = chip * 2 + (1 - core)

    def peer(d):
        return lax.rem(chip + 4 + d, 4) * 2 + core

    mine = pl.ds(pl.multiple_of(lax.axis_index("fs") * ROWS, ROWS), ROWS)
    pairs = (
        (query_ref, narrow.at[0], 0),
        (key_ref, narrow.at[1], 0),
        (forget_ref, narrow.at[2], 0),
        (content_ref, whole.at[mine, pl.ds(128, 128)], 1),
        (switch_ref, whole.at[mine, pl.ds(256, 128)], 1),
        (mix_ref, whole.at[mine, pl.ds(512, 128)], 2),
        (value_ref, whole.at[mine, pl.ds(640, 512)], 3),
        (gate_ref, whole.at[mine, pl.ds(1152, 512)], 3),
        (down_ref, whole.at[mine, pl.ds(1664, 512)], 3),
        (x_ref, x_all.at[tp], 4),
        (pre_ref, pre_gain, 5),
        (post_ref, post_gain, 6),
        (shift_ref, shift_row, 7),
        (spike_ref, spike_turned, 8),
        (unit_ref, unit_row, 9),
        (value_taps_ref, value_taps, 10),
        (gate_taps_ref, gate_taps, 11),
    )
    own = [pltpu.make_async_copy(a, b, own_sem.at[i]) for a, b, i in pairs]
    for one in own[:10]:
        one.start()
    barrier = pltpu.get_barrier_semaphore()
    for axis in ("y", "z"):
        for sign in (1, -1):
            pl.semaphore_signal(
                barrier, inc=1, device_id=neighbour(axis, sign), device_id_type=MESH
            )
    for other in (peer(1), peer(3), partner):
        pl.semaphore_signal(barrier, inc=1, device_id={"tp": other}, device_id_type=MESH)
    for one in own[10:]:
        one.start()

    def landed(at, number):
        pltpu.make_async_copy(at, at, own_sem.at[number]).wait()

    landed(narrow, 0)
    whole[mine, 0:128] = jnp.concatenate((narrow[0], narrow[1]), axis=1)
    whole[mine, 384:512] = jnp.concatenate((narrow[2], jnp.zeros_like(narrow[2])), axis=1)
    landed(whole.at[mine, pl.ds(128, 256)], 1)
    own[5].wait()
    pl.semaphore_wait(barrier, 7)

    def copy_of(m, step):
        o = dict(m["o"])
        o[m["axis"]] = o[m["axis"]] + step * m["sign"]
        row = pl.multiple_of(block_of(o) * ROWS + m["r0"], 16)
        at = whole.at[pl.ds(row, m["rn"]), pl.ds(m["lo"], m["hi"] - m["lo"])]
        return pltpu.make_async_remote_copy(
            src_ref=at,
            dst_ref=at,
            send_sem=send_sem.at[0],
            recv_sem=recv_sem.at[m["sem"]],
            device_id=neighbour(m["axis"], m["sign"]),
            device_id_type=MESH,
        )

    seen, waiting, ahead = set(), list(order), [AHEAD_FIRST]

    def arrived(m):
        if m["sem"] not in seen:
            seen.add(m["sem"])
            at = whole.at[pl.ds(0, m["together"]), pl.ds(m["lo"], m["hi"] - m["lo"])]
            pltpu.make_async_remote_copy(
                src_ref=at,
                dst_ref=at,
                send_sem=send_sem.at[0],
                recv_sem=recv_sem.at[m["sem"]],
                device_id=neighbour(m["axis"], m["sign"]),
                device_id_type=MESH,
            ).wait_recv()

    def pump(until):
        later = []
        for m in waiting:
            if m["start"] > until + ahead[0] or m["ready"] > until:
                later.append(m)
                continue
            for d in m["deps"]:
                arrived(d)
            copy_of(m, 0).start()
        waiting[:] = later

    def class_arrived(cls):
        mine_of = sorted((m for m in order if m["cls"] == cls), key=lambda m: m["arrive"])
        for m in mine_of:
            if m["final"]:
                pump(m["arrive"])
                arrived(m)
        return mine_of[-1]["arrive"]

    def from_depth(cls, dz):
        came = [m for m in order if m["cls"] == cls and m["dz"] == dz]
        for m in sorted(came, key=lambda m: m["arrive"]):
            if m["final"]:
                pump(m["arrive"])
                arrived(m)

    def tp_copy(src, dst, number, to):
        return pltpu.make_async_remote_copy(
            src_ref=src,
            dst_ref=dst,
            send_sem=tp_send.at[number // 10],
            recv_sem=tp_recv.at[number // 10 * 7 + number % 10],
            device_id={"tp": to},
            device_id_type=MESH,
        )

    def begin(copy):
        copy.start()

    right, left = peer(1), peer(3)
    low, high = pl.ds(0, LENGTH // 2), pl.ds(LENGTH // 2, LENGTH // 2)

    def move(buf, owner, rows, number, to):
        at = buf.at[owner, rows]
        return tp_copy(at, at, number, to)

    def share(buf, base, clock):
        begin(move(buf, tp, low, base, right))
        begin(move(buf, tp, high, base + 1, left))
        begin(move(buf, tp, high, base + 2, right))
        begin(move(buf, tp, low, base + 3, left))
        begin(tp_copy(buf.at[tp], buf.at[tp], base + 6, partner))
        clock(1.5)
        clock(1.5)
        move(buf, left, low, base, right).wait_recv()
        begin(move(buf, left, low, base + 4, right))
        move(buf, right, high, base + 1, left).wait_recv()
        begin(move(buf, right, high, base + 5, left))
        clock(1.0)
        move(buf, left, high, base + 2, right).wait_recv()
        begin(tp_copy(buf.at[left], buf.at[left], base + 6, partner))
        move(buf, right, low, base + 3, left).wait_recv()
        begin(tp_copy(buf.at[right], buf.at[right], base + 6, partner))
        clock(1.0)
        clock(1.0)
        far = peer(2)
        move(buf, far, low, base + 4, right).wait_recv()
        move(buf, far, high, base + 5, left).wait_recv()
        begin(tp_copy(buf.at[far], buf.at[far], base + 6, partner))
        clock(1.0)
        came = buf.at[pl.ds(0, 4)]
        tp_copy(came, came, base + 6, partner).wait_recv()

    def summed(product, sums, got, paired, through, joined, chips, base, clock):
        def products(d):
            there = lax.rem(chip + d, 4) * 2
            sums[there + 1 - core] = product(there + 1 - core).astype(bf16)
            sums[there + core] = product(there + core).astype(bf16)
            return tp_copy(sums.at[there + 1 - core], got.at[d], base + d, partner)

        def pair(d):
            there = lax.rem(chip + d, 4) * 2 + core
            tp_copy(sums.at[there], got.at[d], base + d, partner).wait_recv()
            paired[d - 1] = (sums[there].astype(f32) + got[d].astype(f32)).astype(bf16)

        for d in (2, 1, 3, 0):
            begin(products(d))
            clock(0.25)
        clock(0.25)
        pair(2)
        begin(tp_copy(paired.at[1, low], through.at[0], base + 4, right))
        begin(tp_copy(paired.at[1, high], through.at[1], base + 5, left))
        clock(0.5)
        pair(1)
        pair(3)
        begin(tp_copy(paired.at[0, high], chips.at[0, high], base + 6, right))
        tp_copy(sums.at[tp], got.at[0], base, partner).wait_recv()
        total = sums[tp].astype(f32) + got[0].astype(f32)
        begin(tp_copy(paired.at[2, low], chips.at[1, low], base + 6, left))
        clock(1.2)
        clock(1.2)
        tp_copy(through.at[0], through.at[0], base + 4, right).wait_recv()
        half = LENGTH // 2
        joined[0] = (paired[0, 0:half].astype(f32) + through[0].astype(f32)).astype(bf16)
        tp_copy(through.at[1], through.at[1], base + 5, left).wait_recv()
        joined[1] = (paired[2, half:].astype(f32) + through[1].astype(f32)).astype(bf16)
        begin(tp_copy(joined.at[0], chips.at[0, low], base + 6, right))
        begin(tp_copy(joined.at[1], chips.at[1, high], base + 6, left))
        clock(1.3)
        clock(1.3)
        tp_copy(chips, chips, base + 6, right).wait_recv()
        return total + chips[0].astype(f32) + chips[1].astype(f32)

    ticks = [0.5]

    def tick(step):
        ticks[0] = ticks[0] + PACE * step
        pump(ticks[0])

    def still(step):
        del step

    pump(0.0)
    landed(whole.at[mine, pl.ds(640, 1536)], 3)
    own[9].wait()
    share(x_all, 0, tick)
    for one in own[10:]:
        one.wait()
    rows_norm(x_all, pre_gain, normed)
    ticks[0] = class_arrived(0)
    ahead[0] = AHEAD
    pump(ticks[0])

    first = jnp.dot(normed[...], whole[:, 0:256], preferred_element_type=f32)
    second = jnp.dot(normed[...], whole[:, 256:512], preferred_element_type=f32)
    tick(0.7)
    rounded = first.astype(bf16).astype(f32)
    query = rounded[:, 0:64] * HEAD_K ** (-0.5)
    key = rounded[:, 64:128]
    value = rounded[:, 128:256]
    gate = second[:, 0:128].astype(bf16).astype(f32)
    forget = second[:, 128:192] + shift_row[...]
    decay = -(jnp.maximum(-forget, 0.0) + jnp.log1p(jnp.exp(-jnp.abs(forget)))) / 16.0
    decay = decay + spike_turned[...].T
    unit = unit_row[...].astype(f32)
    for piece in attention_pieces(
        query, key, value, gate, decay, unit, lambda a, s: pltpu.roll(a, s, 0)
    ):
        tick(T_PIECE)
        gated = piece

    def mix_part(t):
        rows = pl.ds(pl.multiple_of(t * COLS, COLS), COLS)
        return lax.dot_general(
            gated, whole[rows, 512:640], (((1,), (1,)), ((), ())), preferred_element_type=f32
        )

    total = summed(
        mix_part, sums, from_partner, pair_sums, passing, passed, from_chips, 10, tick
    )
    mix = total.astype(bf16)
    mid_all[tp] = (x_all[tp].astype(f32) + mix.astype(f32)).astype(bf16)
    share(mid_all, 20, tick)
    rows_norm(mid_all, post_gain, normed)
    last_of = {}
    for m in order:
        if m["cls"] == 1:
            last_of[m["dz"]] = max(last_of.get(m["dz"], 0.0), m["arrive"])
    by_arrival = sorted(last_of, key=last_of.get)
    for dz in by_arrival:
        from_depth(1, dz)
        z = lax.rem(lax.axis_index("fs") // 4 + 16 - dz, 8)
        deep = pl.ds(pl.multiple_of(z * 256, 256), 256)
        for at in (0, 512):
            part = jnp.dot(
                normed[:, deep], whole[deep, 640 + at : 1152 + at], preferred_element_type=f32
            )
            if dz == by_arrival[0]:
                raised[:, at : at + 512] = part
            else:
                raised[:, at : at + 512] = raised[:, at : at + 512] + part
    class_arrived(1)
    pump(1e9)

    for block in range(4):
        at = block * 128
        cols = slice(at, at + 128)
        up_value = raised[:, at : at + 128]
        up_gate = raised[:, 512 + at : 640 + at]
        conv_value = short_conv(up_value.astype(bf16).astype(f32), value_taps[:, cols].astype(f32))
        conv_gate = short_conv(up_gate.astype(bf16).astype(f32), gate_taps[:, cols].astype(f32))
        cube = conv_gate + 0.044715 * (conv_gate * conv_gate * conv_gate)
        gelu = conv_gate * (0.5 * (1.0 + jnp.tanh(GELU * cube)))
        hidden[:, cols] = (conv_value * gelu).astype(bf16)

    def down_part(t):
        rows = pl.ds(pl.multiple_of(t * COLS, COLS), COLS)
        return lax.dot_general(
            hidden[...], whole[rows, 1664:2176], (((1,), (1,)), ((), ())), preferred_element_type=f32
        )

    total = summed(
        down_part,
        down_sums,
        down_from_partner,
        down_pair_sums,
        down_passing,
        down_passed,
        down_from_chips,
        30,
        still,
    )
    out_ref[...] = (mid_all[tp].astype(f32) + total.astype(bf16).astype(f32)).astype(bf16)

    seven = x_all.at[pl.ds(0, 7)]
    for group in range(4):
        tp_copy(seven, seven, group * 10, partner).wait_send()
    rest = whole.at[pl.ds(0, 31 * ROWS)]
    pltpu.make_async_remote_copy(
        src_ref=rest,
        dst_ref=rest,
        send_sem=send_sem.at[0],
        recv_sem=recv_sem.at[0],
        device_id=neighbour("y", 1),
        device_id_type=MESH,
    ).wait_send()


T_PIECE = 0.5
AHEAD_FIRST = 1.0
AHEAD = 3.0
PACE = 1.4


def shards(
    incoming_features,
    attend_prenormal_scale,
    probe_matrix,
    lookup_matrix,
    content_matrix,
    forgetting_matrix,
    result_switch_matrix,
    forgetting_shift,
    spike_forget_logarithm,
    attend_unit_scale,
    attend_result_matrix,
    perceptron_scale,
    content_expand_matrix,
    switch_expand_matrix,
    content_kernel,
    switch_kernel,
    contract_matrix,
):
    order = plan(PARTS, 46.6e3, 1.8, 0.02)
    count = 1 + max(m["sem"] for m in order)
    block = (LENGTH, COLS)
    dma = pltpu.SemaphoreType.DMA
    vmem = pl.BlockSpec(memory_space=pltpu.VMEM)
    hbm = pl.BlockSpec(memory_space=pltpu.HBM)
    bf16 = jnp.bfloat16
    return pl.pallas_call(
        functools.partial(layer_kernel, order),
        out_shape=jax.ShapeDtypeStruct(block, bf16),
        in_specs=[hbm] * 17,
        out_specs=vmem,
        scratch_shapes=[
            pltpu.VMEM((32 * ROWS, WIDTH), bf16),
            pltpu.VMEM((GROUP, *block), bf16),
            pltpu.VMEM((GROUP, *block), bf16),
            pltpu.VMEM((GROUP, *block), bf16),
            pltpu.VMEM((4, *block), bf16),
            pltpu.VMEM((3, *block), bf16),
            pltpu.VMEM((2, LENGTH // 2, COLS), bf16),
            pltpu.VMEM((2, LENGTH // 2, COLS), bf16),
            pltpu.VMEM((2, *block), bf16),
            pltpu.VMEM((4, *block), bf16),
            pltpu.VMEM((3, *block), bf16),
            pltpu.VMEM((2, LENGTH // 2, COLS), bf16),
            pltpu.VMEM((2, LENGTH // 2, COLS), bf16),
            pltpu.VMEM((2, *block), bf16),
            pltpu.VMEM((GROUP, *block), bf16),
            pltpu.VMEM((LENGTH, GROUP * COLS), bf16),
            pltpu.VMEM((LENGTH, 512), bf16),
            pltpu.VMEM((LENGTH, 1024), jnp.float32),
            pltpu.VMEM((3, ROWS, 64), bf16),
            pltpu.VMEM((2048,), bf16),
            pltpu.VMEM((2048,), bf16),
            pltpu.VMEM((1, 64), jnp.float32),
            pltpu.VMEM((64, LENGTH), jnp.float32),
            pltpu.VMEM((1, 128), bf16),
            pltpu.VMEM((3, 512), bf16),
            pltpu.VMEM((3, 512), bf16),
            dma((12,)),
            dma((1,)),
            dma((count,)),
            dma((4,)),
            dma((28,)),
        ],
        compiler_params=pltpu.CompilerParams(
            collective_id=0, has_side_effects=True, vmem_limit_bytes=67043328
        ),
    )(
        probe_matrix,
        lookup_matrix,
        content_matrix,
        result_switch_matrix,
        forgetting_matrix,
        attend_result_matrix.T,
        content_expand_matrix,
        switch_expand_matrix,
        contract_matrix.T,
        incoming_features,
        attend_prenormal_scale,
        perceptron_scale,
        forgetting_shift[None],
        spike_forget_logarithm.T,
        attend_unit_scale[None],
        content_kernel,
        switch_kernel,
    )


def solution(mesh):
    placed = (
        P(("rep", "fs"), "tp"),
        P(),
        P("fs", "tp"),
        P("fs", "tp"),
        P("fs", "tp"),
        P("fs", "tp"),
        P("fs", "tp"),
        P("tp"),
        P(("rep", "fs"), "tp"),
        P("tp"),
        P("tp", "fs"),
        P(),
        P("fs", "tp"),
        P("fs", "tp"),
        P(None, "tp"),
        P(None, "tp"),
        P("tp", "fs"),
    )
    return jax.shard_map(
        shards, mesh=mesh, in_specs=placed, out_specs=P(("rep", "fs"), "tp"), check_vma=False
    )
```
